32 devices in a mesh: rep: 2 (over y), fs: 4 (over z), tp: 4 (over x, core).
Axes of the slice: x: 2, y: 2, z: 4, core: 2. Of those that a mesh axis runs over, the one named last changes fastest.
Arguments:
- tokens: bfloat16 [4096, 2048], P(('rep', 'fs'), 'tp'), may hold values from -6 to 6
- outer_gate: float32 [2048, 512], P('fs', 'tp'), may hold values from -0.125 to 0.125
- inner_gate: float32 [2048, 512], P('fs', 'tp'), may hold values from -0.125 to 0.125
- mixer_value: float32 [2048, 512], P('fs', 'tp'), may hold values from -0.125 to 0.125
- mixer_scales: float32 [3, 512], P(None, 'tp'), may hold values from 0.5 to 2
- mixer_taps: float32 [3, 512], P(None, 'tp'), may hold values from -3.5 to 3.5
- mixer_out: float32 [512, 2048], P('fs', 'tp'), may hold values from -0.25 to 0.25
- out_scale: float32 [2048], P('tp'), may hold values from 0.3 to 3
- first_gain: float32 [2048], replicated, may hold values from 0.1 to 1.9
- first_shift: float32 [2048], replicated, may hold values from -2 to 2
- up_proj: float32 [2048, 3072], P('fs', 'tp'), may hold values from -0.125 to 0.125
- gate_proj: float32 [2048, 3072], P('fs', 'tp'), may hold values from -0.125 to 0.125
- up_scales: float32 [2, 3072], P(None, 'tp'), may hold values from 0.5 to 2
- ffn_taps: float32 [3, 2, 3072], P(None, None, 'tp'), may hold values from -3.5 to 3.5
- ffn_shift: float32 [2, 3072], P(None, 'tp'), may hold values from -3 to 3
- down_proj: float32 [3072, 2048], P('fs', 'tp'), may hold values from -0.109375 to 0.109375
- down_scale: float32 [2048], P('tp'), may hold values from 0.3 to 3
- second_gain: float32 [2048], replicated, may hold values from 0.1 to 1.9
- second_shift: float32 [2048], replicated, may hold values from -2 to 2
Outputs:
- layer_out: bfloat16 [4096, 2048], P(('rep', 'fs'), 'tp')
The draws below stay inside these ranges and needn't reach their ends.
All inputs are finite; a program needn't handle non-finite values.
Results may differ from the reference program's by a relative error of at most 0.017.
Values may be sent and summed in bfloat16 or wider, within the bound.
A program may use at most 64 MiB of HBM per device.

```python
import math
import jax
import jax.numpy as jnp
from jax import lax

D = 2048
CW = 512
FF = 3072
LEN = 128
TOKENS = 4096


def shard_levels(rng, shape, split, low, largest):
    def one(position, parts):
        heights = jax.random.uniform(jax.random.fold_in(jax.random.fold_in(rng, 6), position), (parts,), jnp.float32, low / len(split), largest / len(split))
        return jnp.repeat(jnp.exp(heights), shape[position] // parts).reshape((-1,) + (1,) * (len(shape) - position - 1))

    level = one(*split[0])
    for cut in split[1:]:
        level = level * one(*cut)
    return level


def centred(key, dims, width, bound, split=(), kind=jnp.bfloat16):
    array = jax.random.normal(key, dims, jnp.float32) * width
    if len(split) > 0:
        array = shard_levels(key, dims, split, -0.22, 0.18) * array
    return jnp.clip(array, min=-bound, max=bound).astype(kind)


def setup_inputs(seed: int = 0) -> dict:
    key_list = jax.random.split(jax.random.key(seed), 20)
    tokens = centred(key_list[0], (TOKENS, D), 1.0, 6.0, ((0, 8), (1, 4)))
    outer_gate = centred(key_list[1], (D, CW), D ** -0.5, 0.125, ((0, 4), (1, 4)), jnp.float32)
    inner_gate = centred(key_list[2], (D, CW), D ** -0.5, 0.125, ((0, 4), (1, 4)), jnp.float32)
    mixer_value = centred(key_list[3], (D, CW), D ** -0.5, 0.125, ((0, 4), (1, 4)), jnp.float32)
    mixer_scales = jnp.clip(jnp.exp(math.log(2.0) - 1.3862944 * jax.random.uniform(key_list[4], (3, CW), jnp.float32) ** shard_levels(key_list[4], (3, CW), ((1, 4),), -0.2, 0.2)), 0.5, 2.0)
    mixer_taps = centred(key_list[5], (3, CW), 3 ** -0.5, 3.5, ((1, 4),), jnp.float32)
    mixer_out = centred(key_list[6], (CW, D), CW ** -0.5, 0.25, ((0, 4), (1, 4)), jnp.float32)
    out_scale = jnp.clip(jnp.exp(math.log(3.0) - 2.3025851 * jax.random.uniform(key_list[7], (D,), jnp.float32) ** shard_levels(key_list[7], (D,), ((0, 4),), -0.2, 0.2)), 0.3, 3.0)
    first_gain = jnp.clip(1.0 + 0.18 * jax.random.normal(key_list[8], (D,), jnp.float32), 0.1, 1.9)
    first_shift = centred(key_list[9], (D,), 0.3, 2.0, (), jnp.float32)
    up_proj = centred(key_list[10], (D, FF), D ** -0.5, 0.125, ((0, 4), (1, 4)), jnp.float32)
    gate_proj = centred(key_list[11], (D, FF), D ** -0.5, 0.125, ((0, 4), (1, 4)), jnp.float32)
    up_scales = jnp.clip(jnp.exp(math.log(2.0) - 1.3862944 * jax.random.uniform(key_list[12], (2, FF), jnp.float32) ** shard_levels(key_list[12], (2, FF), ((1, 4),), -0.2, 0.2)), 0.5, 2.0)
    ffn_taps = centred(key_list[13], (3, 2, FF), 3 ** -0.5, 3.5, ((2, 4),), jnp.float32)
    ffn_shift = centred(key_list[14], (2, FF), 0.5, 3.0, ((1, 4),), jnp.float32)
    down_proj = centred(key_list[15], (FF, D), FF ** -0.5, 0.109375, ((0, 4), (1, 4)), jnp.float32)
    down_scale = jnp.clip(jnp.exp(math.log(3.0) - 2.3025851 * jax.random.uniform(key_list[16], (D,), jnp.float32) ** shard_levels(key_list[16], (D,), ((0, 4),), -0.2, 0.2)), 0.3, 3.0)
    second_gain = jnp.clip(1.0 + 0.18 * jax.random.normal(key_list[17], (D,), jnp.float32), 0.1, 1.9)
    second_shift = centred(key_list[18], (D,), 0.3, 2.0, (), jnp.float32)
    return {"tokens": tokens, "outer_gate": outer_gate, "inner_gate": inner_gate, "mixer_value": mixer_value, "mixer_scales": mixer_scales, "mixer_taps": mixer_taps, "mixer_out": mixer_out, "out_scale": out_scale, "first_gain": first_gain, "first_shift": first_shift, "up_proj": up_proj, "gate_proj": gate_proj, "up_scales": up_scales, "ffn_taps": ffn_taps, "ffn_shift": ffn_shift, "down_proj": down_proj, "down_scale": down_scale, "second_gain": second_gain, "second_shift": second_shift}


norm_eps = 1e-05
residual_weight = 8.0 ** 0.25

def causal_mix(signal, kernel_taps):
    sequences = signal.reshape(-1, LEN, signal.shape[-1])
    padded = jnp.pad(sequences, ((0, 0), (2, 0), (0, 0)))
    mixed = kernel_taps[0] * padded[:, :-2] + kernel_taps[1] * padded[:, 1:-1] + kernel_taps[2] * padded[:, 2:]
    return mixed.reshape(signal.shape)

def layer_norm(summed, gain_vector, shift_vector):
    average = lax.optimization_barrier(jnp.mean(summed, -1, keepdims=True))
    spread = lax.optimization_barrier(jnp.mean(jnp.square(summed - average), -1, keepdims=True))
    return (summed - average) * lax.rsqrt(spread + norm_eps) * gain_vector + shift_vector

def lowered(matrix):
    return matrix.astype(jnp.bfloat16)

def project(left_rows, matrix, column_scale):
    return jnp.dot(left_rows, lowered(matrix), preferred_element_type=jnp.float32) * column_scale

def reference(tokens, outer_gate, inner_gate, mixer_value, mixer_scales, mixer_taps, mixer_out, out_scale, first_gain, first_shift, up_proj, gate_proj, up_scales, ffn_taps, ffn_shift, down_proj, down_scale, second_gain, second_shift):
    outer_part = project(tokens, outer_gate, mixer_scales[0]).astype(jnp.bfloat16)
    inner_part = project(tokens, inner_gate, mixer_scales[1]).astype(jnp.bfloat16)
    value_part = project(tokens, mixer_value, mixer_scales[2]).astype(jnp.bfloat16)
    product = inner_part.astype(jnp.float32) * value_part.astype(jnp.float32)
    mixed_conv = (outer_part.astype(jnp.float32) * causal_mix(product, mixer_taps)).astype(jnp.bfloat16)
    mixer_sum = project(mixed_conv, mixer_out, out_scale)
    first_sum = residual_weight * tokens.astype(jnp.float32) + mixer_sum
    normed = layer_norm(first_sum, first_gain, first_shift).astype(jnp.bfloat16)
    up_linear = project(normed, up_proj, up_scales[0])
    gate_linear = project(normed, gate_proj, up_scales[1])
    up_mixed = causal_mix(up_linear, ffn_taps[:, 0]) + ffn_shift[0]
    gate_mixed = causal_mix(gate_linear, ffn_taps[:, 1]) + ffn_shift[1]
    hidden = (up_mixed * jax.nn.silu(gate_mixed)).astype(jnp.bfloat16)
    ffn_sum = project(hidden, down_proj, down_scale)
    second_sum = residual_weight * normed.astype(jnp.float32) + ffn_sum
    return layer_norm(second_sum, second_gain, second_shift).astype(jnp.bfloat16)
```

```python
import functools

import jax
import jax.numpy as jnp
from jax import lax
from jax.experimental import pallas as pl
from jax.experimental.pallas import tpu as pltpu
from jax.sharding import PartitionSpec as P

LEN = 128


norm_eps = 1e-05
residual_weight = 8.0**0.25


def causal_mix(signal, kernel_taps):
    sequences = signal.reshape(-1, LEN, signal.shape[-1])
    padded = jnp.pad(sequences, ((0, 0), (2, 0), (0, 0)))
    mixed = (
        kernel_taps[0] * padded[:, :-2]
        + kernel_taps[1] * padded[:, 1:-1]
        + kernel_taps[2] * padded[:, 2:]
    )
    return mixed.reshape(signal.shape)


def lowered(matrix):
    return matrix.astype(jnp.bfloat16)


def single_fold(operand, portion):
    return jnp.dot(operand, portion, preferred_element_type=jnp.float32)


def fold_step(operand, pieces):
    result = []
    for number in range(len(pieces)):
        result.append(jnp.dot(operand, pieces[number], preferred_element_type=jnp.float32))
    return tuple(result)


def own_columns(vector, own_width):
    return lax.dynamic_slice_in_dim(vector, lax.axis_index("tp") * own_width, own_width, 0)


def scaled_norm(summed, average, spread, gain_vector, shift_vector):
    return (summed - average) * lax.rsqrt(spread + norm_eps) * gain_vector + shift_vector


def local(
    tokens,
    outer_gate,
    inner_gate,
    mixer_value,
    mixer_scales,
    mixer_taps,
    mixer_out,
    out_scale,
    first_gain,
    first_shift,
    up_proj,
    gate_proj,
    up_scales,
    ffn_taps,
    ffn_shift,
    down_proj,
    down_scale,
    second_gain,
    second_shift,
):
    own_width = tokens.shape[1]
    full_width = own_width * lax.axis_size("tp")
    token_whole = lax.all_gather(tokens, "tp", axis=1, tiled=True)
    outer_part, inner_part, value_part = fold_step(
        token_whole,
        (
            lax.all_gather(lowered(outer_gate), "fs", axis=0, tiled=True),
            lax.all_gather(lowered(inner_gate), "fs", axis=0, tiled=True),
            lax.all_gather(lowered(mixer_value), "fs", axis=0, tiled=True),
        ),
    )
    outer_part = (outer_part * mixer_scales[0]).astype(jnp.bfloat16)
    inner_part = (inner_part * mixer_scales[1]).astype(jnp.bfloat16)
    value_part = (value_part * mixer_scales[2]).astype(jnp.bfloat16)
    product = inner_part.astype(jnp.float32) * value_part.astype(jnp.float32)
    mixed_conv = (outer_part.astype(jnp.float32) * causal_mix(product, mixer_taps)).astype(
        jnp.bfloat16
    )
    conv_whole = lax.all_gather(mixed_conv, "tp", axis=1, tiled=True)
    mixer_sum = (
        single_fold(conv_whole, lax.all_gather(lowered(mixer_out), "fs", axis=0, tiled=True))
        * out_scale
    )
    first_sum = residual_weight * tokens.astype(jnp.float32) + mixer_sum
    row_total, row_square = lax.psum(
        (jnp.sum(first_sum, 1, keepdims=True), jnp.sum(first_sum * first_sum, 1, keepdims=True)),
        "tp",
    )
    average = row_total / full_width
    spread = row_square / full_width - average * average
    normed = scaled_norm(
        first_sum,
        average,
        spread,
        own_columns(first_gain, own_width),
        own_columns(first_shift, own_width),
    ).astype(jnp.bfloat16)
    normed_whole = lax.all_gather(normed, "tp", axis=1, tiled=True)
    up_matrix, gate_matrix = (
        lax.all_gather(lowered(up_proj), "fs", axis=0, tiled=True),
        lax.all_gather(lowered(gate_proj), "fs", axis=0, tiled=True),
    )
    up_linear = jnp.dot(normed_whole, up_matrix, preferred_element_type=jnp.float32)
    gate_linear = jnp.dot(normed_whole, gate_matrix, preferred_element_type=jnp.float32)
    up_linear = up_linear * up_scales[0]
    gate_linear = gate_linear * up_scales[1]
    up_mixed = causal_mix(up_linear, ffn_taps[:, 0]) + ffn_shift[0]
    gate_mixed = causal_mix(gate_linear, ffn_taps[:, 1]) + ffn_shift[1]
    hidden = (up_mixed * jax.nn.silu(gate_mixed)).astype(jnp.bfloat16)
    hidden_whole = lax.all_gather(hidden, "tp", axis=1, tiled=True)
    ffn_sum = (
        single_fold(hidden_whole, lax.all_gather(lowered(down_proj), "fs", axis=0, tiled=True))
        * down_scale
    )
    second_sum = residual_weight * normed.astype(jnp.float32) + ffn_sum
    second_total, second_square = lax.psum(
        (jnp.sum(second_sum, 1, keepdims=True), jnp.sum(second_sum * second_sum, 1, keepdims=True)),
        "tp",
    )
    second_average = second_total / full_width
    second_spread = second_square / full_width - second_average * second_average
    return scaled_norm(
        second_sum,
        second_average,
        second_spread,
        own_columns(second_gain, own_width),
        own_columns(second_shift, own_width),
    ).astype(jnp.bfloat16)


LANES = 128
GUEST_PARTS = 2


def shifted_mix(signal, first, second, third):
    rows = lax.broadcasted_iota(jnp.int32, signal.shape, 0) % LEN
    one = jnp.where(rows >= 1, pltpu.roll(signal, 1, 0), 0.0)
    two = jnp.where(rows >= 2, pltpu.roll(signal, 2, 0), 0.0)
    return first * two + second * one + third * signal


def dot32(left, right):
    return jnp.dot(left, right, preferred_element_type=jnp.float32)


def kernel(
    fs,
    tp,
    tokens_hbm,
    outer_hbm,
    inner_hbm,
    value_hbm,
    out_hbm,
    up_hbm,
    gate_hbm,
    down_hbm,
    mixer_scales,
    mixer_taps,
    out_scale,
    first_gain,
    first_shift,
    up_scales,
    ffn_taps,
    ffn_shift,
    down_scale,
    second_gain,
    second_shift,
    result,
    mix_f,
    out_f,
    up_f,
    gate_f,
    down_f,
    mix_g,
    out_g,
    ug_g,
    down_g,
    token_all,
    conv_all,
    norm_all,
    guest_all,
    hidden_all,
    hidden_out,
    first_sum,
    total,
    stats,
    load_sem,
    send_z,
    send_y,
    recv_z,
    recv_y,
    send_x,
    recv_x,
    send_s,
    recv_s,
    send_g,
    recv_g,
    send_h,
    recv_h,
):
    r, z, t = lax.axis_index("rep"), lax.axis_index("fs"), lax.axis_index("tp")
    sibling = t + 1 - 2 * (t % 2)
    across = (t + 2) % tp
    diagonal = (sibling + 2) % tp
    other = 1 - r
    rows, own_width = result.shape
    full_width = own_width * tp
    channels = conv_all.shape[2]
    blocks = ug_g.shape[1]
    last = fs - 1
    own_lanes = pl.ds(pl.multiple_of(t * own_width, own_width), own_width)

    sources = (tokens_hbm, outer_hbm, inner_hbm, value_hbm, out_hbm, up_hbm, gate_hbm, down_hbm)
    places = (token_all.at[t], mix_f.at[0], mix_f.at[1], mix_f.at[2], out_f, up_f, gate_f, down_f)
    loads = [
        pltpu.make_async_copy(source, place, load_sem.at[number])
        for number, (source, place) in enumerate(zip(sources, places))
    ]
    for load in loads:
        load.start()

    barrier = pltpu.get_barrier_semaphore()
    for peer in (sibling, across, diagonal):
        pl.semaphore_signal(barrier, inc=1, device_id={"tp": peer}, device_id_type=pl.DeviceIdType.MESH)
    pl.semaphore_signal(barrier, inc=1, device_id={"rep": other}, device_id_type=pl.DeviceIdType.MESH)

    @pl.when(z > 0)
    def _():
        pl.semaphore_signal(barrier, inc=1, device_id={"fs": z - 1}, device_id_type=pl.DeviceIdType.MESH)

    @pl.when(z < last)
    def _():
        pl.semaphore_signal(barrier, inc=1, device_id={"fs": z + 1}, device_id_type=pl.DeviceIdType.MESH)

    inside = (z > 0) & (z < last)

    @pl.when(inside)
    def _():
        pl.semaphore_wait(barrier, 6)

    @pl.when(jnp.logical_not(inside))
    def _():
        pl.semaphore_wait(barrier, 5)

    def hop(number, slot, ref, peer, kind):
        return pltpu.make_async_remote_copy(
            src_ref=ref(slot),
            dst_ref=ref(slot),
            send_sem=send_x.at[number, kind],
            recv_sem=recv_x.at[number, slot],
            device_id={"tp": peer},
            device_id_type=pl.DeviceIdType.MESH,
        )

    def token_block(slot):
        return token_all.at[slot]

    def conv_block(slot):
        return conv_all.at[slot]

    def norm_block(slot):
        return norm_all.at[slot]

    def hidden_block(number):
        return lambda slot: hidden_all.at[slot, number]

    guest_rows = rows // GUEST_PARTS

    def guest_block(part):
        return lambda slot: guest_all.at[slot, pl.ds(part * guest_rows, guest_rows)]

    exchanges = [token_block, conv_block, norm_block]
    exchanges += [hidden_block(block) for block in range(blocks)]
    exchanges += [guest_block(part) for part in range(GUEST_PARTS)]
    first_hidden, first_guest = 3, 3 + blocks

    def mix_unit(part):
        size = mix_g.shape[1] // 4
        return lambda source, half: mix_g.at[source, pl.ds(pl.multiple_of((part * 2 + half) * size, size), size)]

    def out_unit(source, half):
        size = out_g.shape[1] // 2
        return out_g.at[source, pl.ds(pl.multiple_of(half * size, size), size)]

    def ug_unit(block):
        size = ug_g.shape[2] // 2
        return lambda source, half: ug_g.at[source, block, pl.ds(pl.multiple_of(half * size, size), size)]

    def down_unit(part):
        size = LANES
        return lambda source, half: down_g.at[source, pl.ds(pl.multiple_of((part * 2 + half) * size, size), size)]

    parts = blocks // 2
    units = [mix_unit(0), mix_unit(1), out_unit]
    units += [down_unit(part) for part in range(parts)]
    units += [ug_unit(block) for block in range(blocks)]
    count = len(units)
    first_down, first_ug = 3, 3 + parts
    whole = [True] * 3 + [False] * (parts - 1) + [True] + [True] * blocks

    def summing(number, peer, slot, kind):
        return pltpu.make_async_remote_copy(
            src_ref=stats.at[number, slot],
            dst_ref=stats.at[number, slot],
            send_sem=send_s.at[number, kind],
            recv_sem=recv_s.at[number, slot],
            device_id={"tp": peer},
            device_id_type=pl.DeviceIdType.MESH,
        )

    def program(middle):
        if middle:
            outer, inner, far = (z - 1) * last, last - z, (2 - z) * last
        else:
            near = 1 + z // last
            beyond, far = last - near, last - z
        sent = []

        def begin(copy):
            copy.start()
            sent.append(copy)

        def exchange_start(number):
            begin(hop(number, t, exchanges[number], across, 0))
            begin(hop(number, t, exchanges[number], sibling, 1))

        def exchange_pass(number):
            hop(number, across, exchanges[number], across, 0).wait_recv()
            begin(hop(number, across, exchanges[number], sibling, 2))

        def exchange_end(number):
            hop(number, sibling, exchanges[number], sibling, 1).wait_recv()
            hop(number, diagonal, exchanges[number], sibling, 2).wait_recv()

        def along(unit, source, target, way, kind):
            ref = units[unit](source, other if kind else r)
            return pltpu.make_async_remote_copy(
                src_ref=ref,
                dst_ref=ref,
                send_sem=send_z.at[unit, source, way, kind],
                recv_sem=recv_z.at[unit, source, kind],
                device_id={"fs": target},
                device_id_type=pl.DeviceIdType.MESH,
            )

        def over(unit, source, half):
            ref = units[unit](source, half)
            return pltpu.make_async_remote_copy(
                src_ref=ref,
                dst_ref=ref,
                send_sem=send_y.at[unit, source],
                recv_sem=recv_y.at[unit, source],
                device_id={"rep": other},
                device_id_type=pl.DeviceIdType.MESH,
            )

        def own(unit):
            if middle:
                begin(along(unit, z, inner, 0, 0))
                if unit < first_ug:
                    begin(along(unit, z, outer, 1, 0))
            else:
                begin(along(unit, z, near, 0, 0))

        def own_rest(unit):
            if whole[unit]:
                begin(along(unit, z, near, 0, 1))

        def from_outer(unit):
            along(unit, outer, z, 0, 0).wait_recv()
            begin(along(unit, outer, inner, 0, 0))
            if not whole[unit]:
                begin(over(unit, outer, r))

        def from_inner(unit, source):
            along(unit, source, z, 0, 0).wait_recv()
            begin(over(unit, source, r))
            if middle and unit < first_ug:
                begin(along(unit, source, outer, 1, 0))

        def need(unit):
            if middle:
                if whole[unit]:
                    along(unit, outer, z, 0, 1).wait_recv()
                else:
                    over(unit, outer, other).wait_recv()
                over(unit, inner, other).wait_recv()
                over(unit, far, other).wait_recv()
            else:
                for source in (near, beyond, far):
                    over(unit, source, other).wait_recv()

        def lower_mix():
            for part in range(3):
                mix_g[z, :, part * channels : (part + 1) * channels] = mix_f[part].astype(jnp.bfloat16)

        def lower_block(block):
            columns = slice(block * LANES, (block + 1) * LANES)
            ug_g[z, block, :, :LANES] = up_f[:, columns].astype(jnp.bfloat16)
            ug_g[z, block, :, LANES:] = gate_f[:, columns].astype(jnp.bfloat16)

        def sums_start(number, summed):
            lane = lax.broadcasted_iota(jnp.int32, (rows, LANES), 1)
            one = jnp.sum(summed, axis=1, keepdims=True)
            two = jnp.sum(summed * summed, axis=1, keepdims=True)
            stats[number, t] = jnp.transpose(jnp.where(lane == 0, one, two))[:8]
            for kind, peer in enumerate((across, diagonal, sibling)):
                begin(summing(number, peer, t, kind))

        def sums_end(number):
            for kind, peer in enumerate((across, diagonal, sibling)):
                summing(number, peer, peer, kind).wait_recv()
            summed = stats[number, 0]
            for slot in range(1, tp):
                summed = summed + stats[number, slot]
            back = jnp.transpose(jnp.concatenate([summed] * (LANES // 8), axis=0))
            average = back[:, 0:1] / full_width
            return average, back[:, 1:2] / full_width - average * average

        def mixer():
            for unit in (0, 1):
                need(unit)
            exchange_end(0)
            gathered = dot32(token_all[0], mix_g[0])
            for slot in range(1, tp):
                gathered = gathered + dot32(token_all[slot], mix_g[slot])
            scaled = [
                (gathered[:, part * channels : (part + 1) * channels] * mixer_scales[part : part + 1])
                .astype(jnp.bfloat16)
                .astype(jnp.float32)
                for part in range(3)
            ]
            mixed = scaled[0] * shifted_mix(
                scaled[1] * scaled[2], mixer_taps[0:1], mixer_taps[1:2], mixer_taps[2:3]
            )
            conv_all[t] = mixed.astype(jnp.bfloat16)
            exchange_start(1)

        def mixer_output():
            need(2)
            exchange_end(1)
            summed = dot32(conv_all[0], out_g[0])
            for slot in range(1, tp):
                summed = summed + dot32(conv_all[slot], out_g[slot])
            summed = summed * out_scale[...] + residual_weight * token_all[t].astype(jnp.float32)
            first_sum[...] = summed
            sums_start(0, summed)

        def first_norm():
            average, spread = sums_end(0)
            norm_all[t] = scaled_norm(
                first_sum[...], average, spread, first_gain[:, own_lanes], first_shift[:, own_lanes]
            ).astype(jnp.bfloat16)

        def guest_copy(part):
            lines = pl.ds(part * guest_rows, guest_rows)
            return pltpu.make_async_remote_copy(
                src_ref=norm_all.at[t, lines],
                dst_ref=guest_all.at[t, lines],
                send_sem=send_g.at[part],
                recv_sem=recv_g.at[part],
                device_id={"fs": outer if middle else near},
                device_id_type=pl.DeviceIdType.MESH,
            )

        def hidden_copy(block):
            return pltpu.make_async_remote_copy(
                src_ref=hidden_out.at[block],
                dst_ref=hidden_all.at[t, block],
                send_sem=send_h.at[block],
                recv_sem=recv_h.at[block],
                device_id={"fs": outer if middle else near},
                device_id_type=pl.DeviceIdType.MESH,
            )

        def units_of(block, left):
            both = dot32(left[0], ug_g[0, block])
            for slot in range(1, tp):
                both = both + dot32(left[slot], ug_g[slot, block])
            columns = slice(block * LANES, (block + 1) * LANES)
            mixed = []
            for side in range(2):
                mixed.append(
                    shifted_mix(
                        both[:, side * LANES : (side + 1) * LANES] * up_scales[side : side + 1, columns],
                        ffn_taps[0, side : side + 1, columns],
                        ffn_taps[1, side : side + 1, columns],
                        ffn_taps[2, side : side + 1, columns],
                    )
                    + ffn_shift[side : side + 1, columns]
                )
            return (mixed[0] * mixed[1] / (1.0 + jnp.exp(-mixed[1]))).astype(jnp.bfloat16)

        def hidden(block):
            hidden_all[t, block] = units_of(block, norm_all)
            exchange_start(first_hidden + block)

        def guest_hidden(block):
            hidden_out[block] = units_of(block, guest_all)
            begin(hidden_copy(block))

        def guest_start(part):
            guest_copy(part).wait_recv()
            exchange_start(first_guest + part)

        def returned(block):
            hidden_copy(block).wait_recv()
            exchange_start(first_hidden + block)

        def down(part):
            need(first_down + part)
            for block in (2 * part, 2 * part + 1):
                exchange_end(first_hidden + block)
            summed = None
            for slot in range(tp):
                left = jnp.concatenate([hidden_all[slot, 2 * part], hidden_all[slot, 2 * part + 1]], axis=1)
                term = dot32(left, down_g[slot, part * 2 * LANES : (part + 1) * 2 * LANES])
                summed = term if summed is None else summed + term
            total[...] = summed if part == 0 else total[...] + summed

        def finish():
            second = total[...] * down_scale[...] + residual_weight * norm_all[t].astype(jnp.float32)
            total[...] = second
            sums_start(1, second)
            for copy in sent[:-3]:
                copy.wait_send()
            average, spread = sums_end(1)
            result[...] = scaled_norm(
                total[...], average, spread, second_gain[:, own_lanes], second_shift[:, own_lanes]
            ).astype(result.dtype)
            for copy in sent[-3:]:
                copy.wait_send()

        def sources_of(unit):
            from_outer(unit)
            from_inner(unit, inner)

        loads[0].wait()
        exchange_start(0)
        for load in loads[1:4]:
            load.wait()
        lower_mix()
        d, u, h, g = first_down, first_ug, first_hidden, first_guest
        if middle:
            own(0)
            own(1)
            loads[4].wait()
            out_g[z] = out_f[...].astype(jnp.bfloat16)
            own(2)
            loads[7].wait()
            down_g[z] = down_f[...].astype(jnp.bfloat16)
            own(d)
            sources_of(0)
            loads[5].wait()
            loads[6].wait()
            lower_block(0)
            lower_block(1)
            own(d + 1)
            sources_of(1)
            from_inner(0, far)
            lower_block(2)
            lower_block(3)
            sources_of(2)
            from_inner(1, far)
            own(d + 2)
            exchange_pass(0)
            lower_block(4)
            lower_block(5)
            from_inner(2, far)
            sources_of(d)
            mixer()
            own(u)
            from_inner(d, far)
            sources_of(d + 1)
            exchange_pass(1)
            mixer_output()
            own(u + 1)
            from_inner(d + 1, far)
            sources_of(d + 2)
            first_norm()
            exchange_start(2)
            own(u + 2)
            from_inner(d + 2, far)
            sources_of(u)
            from_inner(u, far)
            own(u + 3)
            guest_start(0)
            sources_of(u + 1)
            exchange_pass(2)
            exchange_end(2)
            guest_start(1)
            from_inner(u + 1, far)
            own(u + 4)
            need(u)
            hidden(0)
            sources_of(u + 2)
            exchange_pass(g)
            from_inner(u + 2, far)
            own(u + 5)
            need(u + 1)
            hidden(1)
            exchange_pass(g + 1)
            sources_of(u + 3)
            exchange_end(g)
            exchange_end(g + 1)
            guest_hidden(0)
            guest_hidden(1)
            from_inner(u + 3, far)
            exchange_pass(h)
            need(u + 2)
            guest_hidden(2)
            hidden(2)
            exchange_pass(h + 1)
            sources_of(u + 4)
            from_inner(u + 4, far)
            need(u + 3)
            guest_hidden(3)
            hidden(3)
            sources_of(u + 5)
            exchange_pass(h + 2)
            from_inner(u + 5, far)
            need(u + 4)
            guest_hidden(4)
            hidden(4)
            exchange_pass(h + 3)
            down(0)
            need(u + 5)
            guest_hidden(5)
            hidden(5)
            down(1)
            exchange_pass(h + 4)
            exchange_pass(h + 5)
            down(2)
            finish()
        else:
            own(0)
            own_rest(0)
            own(1)
            own_rest(1)
            loads[4].wait()
            out_g[z] = out_f[...].astype(jnp.bfloat16)
            own(2)
            own_rest(2)
            loads[7].wait()
            down_g[z] = down_f[...].astype(jnp.bfloat16)
            for part in range(parts):
                own(d + part)
                own_rest(d + part)
            loads[5].wait()
            loads[6].wait()
            for block in range(blocks):
                lower_block(block)
            own(u)
            own_rest(u)
            from_inner(0, near)
            from_inner(1, near)
            from_inner(0, beyond)
            from_inner(0, far)
            from_inner(1, beyond)
            exchange_pass(0)
            from_inner(1, far)
            from_inner(2, near)
            from_inner(2, beyond)
            from_inner(2, far)
            mixer()
            from_inner(d, near)
            from_inner(d, beyond)
            exchange_pass(1)
            mixer_output()
            first_norm()
            for part in range(GUEST_PARTS):
                begin(guest_copy(part))
            own(u + 1)
            for block in range(1, blocks):
                if block + 1 < blocks:
                    own(u + block + 1)
                own_rest(u + block)
            from_inner(d, far)
            for part in range(1, parts):
                for source in (near, beyond, far):
                    from_inner(d + part, source)
            for block in range(blocks):
                returned(block)
                if block > 0:
                    exchange_pass(h + block - 1)
                if block > 2 and block % 2 == 0:
                    down(block // 2 - 2)
            exchange_pass(h + blocks - 1)
            for part in range(max(parts - 2, 0), parts):
                down(part)
            finish()

    @pl.when(inside)
    def _():
        program(True)

    @pl.when(jnp.logical_not(inside))
    def _():
        program(False)


def fused(
    fs,
    tp,
    tokens,
    outer_gate,
    inner_gate,
    mixer_value,
    mixer_scales,
    mixer_taps,
    mixer_out,
    out_scale,
    first_gain,
    first_shift,
    up_proj,
    gate_proj,
    up_scales,
    ffn_taps,
    ffn_shift,
    down_proj,
    down_scale,
    second_gain,
    second_shift,
):
    rows, own_width = tokens.shape
    depth, channels = outer_gate.shape
    hidden = up_proj.shape[1]
    blocks = hidden // LANES
    count = 3 + blocks + blocks // 2
    moves = 3 + blocks + GUEST_PARTS
    any_space = pl.BlockSpec(memory_space=pl.ANY)
    in_vmem = pl.BlockSpec(memory_space=pltpu.VMEM)

    def row(vector):
        return vector.reshape(1, -1)

    return pl.pallas_call(
        functools.partial(kernel, fs, tp),
        out_shape=jax.ShapeDtypeStruct((rows, own_width), jnp.bfloat16),
        in_specs=[any_space] * 8 + [in_vmem] * 11,
        out_specs=in_vmem,
        scratch_shapes=[
            pltpu.VMEM((3, depth, channels), jnp.float32),
            pltpu.VMEM(mixer_out.shape, jnp.float32),
            pltpu.VMEM(up_proj.shape, jnp.float32),
            pltpu.VMEM(gate_proj.shape, jnp.float32),
            pltpu.VMEM(down_proj.shape, jnp.float32),
            pltpu.VMEM((fs, depth, 3 * channels), jnp.bfloat16),
            pltpu.VMEM((fs,) + mixer_out.shape, jnp.bfloat16),
            pltpu.VMEM((fs, blocks, depth, 2 * LANES), jnp.bfloat16),
            pltpu.VMEM((fs,) + down_proj.shape, jnp.bfloat16),
            pltpu.VMEM((tp, rows, own_width), jnp.bfloat16),
            pltpu.VMEM((tp, rows, channels), jnp.bfloat16),
            pltpu.VMEM((tp, rows, own_width), jnp.bfloat16),
            pltpu.VMEM((tp, rows, own_width), jnp.bfloat16),
            pltpu.VMEM((tp, blocks, rows, LANES), jnp.bfloat16),
            pltpu.VMEM((blocks, rows, LANES), jnp.bfloat16),
            pltpu.VMEM((rows, own_width), jnp.float32),
            pltpu.VMEM((rows, own_width), jnp.float32),
            pltpu.VMEM((2, tp, 8, rows), jnp.float32),
            pltpu.SemaphoreType.DMA((8,)),
            pltpu.SemaphoreType.DMA((count, fs, 2, 2)),
            pltpu.SemaphoreType.DMA((count, fs)),
            pltpu.SemaphoreType.DMA((count, fs, 2)),
            pltpu.SemaphoreType.DMA((count, fs)),
            pltpu.SemaphoreType.DMA((moves, 3)),
            pltpu.SemaphoreType.DMA((moves, tp)),
            pltpu.SemaphoreType.DMA((2, 3)),
            pltpu.SemaphoreType.DMA((2, tp)),
            pltpu.SemaphoreType.DMA((GUEST_PARTS,)),
            pltpu.SemaphoreType.DMA((GUEST_PARTS,)),
            pltpu.SemaphoreType.DMA((blocks,)),
            pltpu.SemaphoreType.DMA((blocks,)),
        ],
        compiler_params=pltpu.CompilerParams(
            collective_id=0, has_side_effects=True, vmem_limit_bytes=60 * 1024 * 1024
        ),
    )(
        tokens,
        outer_gate,
        inner_gate,
        mixer_value,
        mixer_out,
        up_proj,
        gate_proj,
        down_proj,
        mixer_scales,
        mixer_taps,
        row(out_scale),
        row(first_gain),
        row(first_shift),
        up_scales,
        ffn_taps,
        ffn_shift,
        row(down_scale),
        row(second_gain),
        row(second_shift),
    )


def fits(mesh):
    return mesh.shape["rep"] == 2 and mesh.shape["fs"] == 4 and mesh.shape["tp"] == 4


def solution(mesh):
    body = functools.partial(fused, mesh.shape["fs"], mesh.shape["tp"]) if fits(mesh) else local
    return jax.shard_map(
        body,
        mesh=mesh,
        in_specs=(
            P(("rep", "fs"), "tp"),
            P("fs", "tp"),
            P("fs", "tp"),
            P("fs", "tp"),
            P(None, "tp"),
            P(None, "tp"),
            P("fs", "tp"),
            P("tp"),
            P(),
            P(),
            P("fs", "tp"),
            P("fs", "tp"),
            P(None, "tp"),
            P(None, None, "tp"),
            P(None, "tp"),
            P("fs", "tp"),
            P("tp"),
            P(),
            P(),
        ),
        out_specs=P(("rep", "fs"), "tp"),
        check_vma=False,
    )
```

```python
import functools

import jax
import jax.numpy as jnp
from jax import lax
from jax.experimental import pallas as pl
from jax.experimental.pallas import tpu as pltpu
from jax.sharding import PartitionSpec as P

LEN = 128


norm_eps = 1e-05
residual_weight = 8.0**0.25


def causal_mix(signal, kernel_taps):
    sequences = signal.reshape(-1, LEN, signal.shape[-1])
    padded = jnp.pad(sequences, ((0, 0), (2, 0), (0, 0)))
    mixed = (
        kernel_taps[0] * padded[:, :-2]
        + kernel_taps[1] * padded[:, 1:-1]
        + kernel_taps[2] * padded[:, 2:]
    )
    return mixed.reshape(signal.shape)


def lowered(matrix):
    return matrix.astype(jnp.bfloat16)


def single_fold(operand, portion):
    return jnp.dot(operand, portion, preferred_element_type=jnp.float32)


def fold_step(operand, pieces):
    result = []
    for number in range(len(pieces)):
        result.append(jnp.dot(operand, pieces[number], preferred_element_type=jnp.float32))
    return tuple(result)


def own_columns(vector, own_width):
    return lax.dynamic_slice_in_dim(vector, lax.axis_index("tp") * own_width, own_width, 0)


def scaled_norm(summed, average, spread, gain_vector, shift_vector):
    return (summed - average) * lax.rsqrt(spread + norm_eps) * gain_vector + shift_vector


def local(
    tokens,
    outer_gate,
    inner_gate,
    mixer_value,
    mixer_scales,
    mixer_taps,
    mixer_out,
    out_scale,
    first_gain,
    first_shift,
    up_proj,
    gate_proj,
    up_scales,
    ffn_taps,
    ffn_shift,
    down_proj,
    down_scale,
    second_gain,
    second_shift,
):
    own_width = tokens.shape[1]
    full_width = own_width * lax.axis_size("tp")
    token_whole = lax.all_gather(tokens, "tp", axis=1, tiled=True)
    outer_part, inner_part, value_part = fold_step(
        token_whole,
        (
            lax.all_gather(lowered(outer_gate), "fs", axis=0, tiled=True),
            lax.all_gather(lowered(inner_gate), "fs", axis=0, tiled=True),
            lax.all_gather(lowered(mixer_value), "fs", axis=0, tiled=True),
        ),
    )
    outer_part = (outer_part * mixer_scales[0]).astype(jnp.bfloat16)
    inner_part = (inner_part * mixer_scales[1]).astype(jnp.bfloat16)
    value_part = (value_part * mixer_scales[2]).astype(jnp.bfloat16)
    product = inner_part.astype(jnp.float32) * value_part.astype(jnp.float32)
    mixed_conv = (outer_part.astype(jnp.float32) * causal_mix(product, mixer_taps)).astype(
        jnp.bfloat16
    )
    conv_whole = lax.all_gather(mixed_conv, "tp", axis=1, tiled=True)
    mixer_sum = (
        single_fold(conv_whole, lax.all_gather(lowered(mixer_out), "fs", axis=0, tiled=True))
        * out_scale
    )
    first_sum = residual_weight * tokens.astype(jnp.float32) + mixer_sum
    row_total, row_square = lax.psum(
        (jnp.sum(first_sum, 1, keepdims=True), jnp.sum(first_sum * first_sum, 1, keepdims=True)),
        "tp",
    )
    average = row_total / full_width
    spread = row_square / full_width - average * average
    normed = scaled_norm(
        first_sum,
        average,
        spread,
        own_columns(first_gain, own_width),
        own_columns(first_shift, own_width),
    ).astype(jnp.bfloat16)
    normed_whole = lax.all_gather(normed, "tp", axis=1, tiled=True)
    up_matrix, gate_matrix = (
        lax.all_gather(lowered(up_proj), "fs", axis=0, tiled=True),
        lax.all_gather(lowered(gate_proj), "fs", axis=0, tiled=True),
    )
    up_linear = jnp.dot(normed_whole, up_matrix, preferred_element_type=jnp.float32)
    gate_linear = jnp.dot(normed_whole, gate_matrix, preferred_element_type=jnp.float32)
    up_linear = up_linear * up_scales[0]
    gate_linear = gate_linear * up_scales[1]
    up_mixed = causal_mix(up_linear, ffn_taps[:, 0]) + ffn_shift[0]
    gate_mixed = causal_mix(gate_linear, ffn_taps[:, 1]) + ffn_shift[1]
    hidden = (up_mixed * jax.nn.silu(gate_mixed)).astype(jnp.bfloat16)
    hidden_whole = lax.all_gather(hidden, "tp", axis=1, tiled=True)
    ffn_sum = (
        single_fold(hidden_whole, lax.all_gather(lowered(down_proj), "fs", axis=0, tiled=True))
        * down_scale
    )
    second_sum = residual_weight * normed.astype(jnp.float32) + ffn_sum
    second_total, second_square = lax.psum(
        (jnp.sum(second_sum, 1, keepdims=True), jnp.sum(second_sum * second_sum, 1, keepdims=True)),
        "tp",
    )
    second_average = second_total / full_width
    second_spread = second_square / full_width - second_average * second_average
    return scaled_norm(
        second_sum,
        second_average,
        second_spread,
        own_columns(second_gain, own_width),
        own_columns(second_shift, own_width),
    ).astype(jnp.bfloat16)


LANES = 128
STAT_ROWS = 8
GUEST_PARTS = 2
RETURN_PARTS = 2
MIX_PARTS = 4
BLOCK_PARTS = (1, 1, 1, 1, 1, 2)
LANE_DEPTH = {"zi": 14, "zo": 8, "y": 8, "x": 8, "d": 8}


def shifted_mix(signal, first, second, third):
    rows = lax.broadcasted_iota(jnp.int32, signal.shape, 0) % LEN
    one = jnp.where(rows >= 1, pltpu.roll(signal, 1, 0), 0.0)
    two = jnp.where(rows >= 2, pltpu.roll(signal, 2, 0), 0.0)
    return first * two + second * one + third * signal


def dot32(left, right):
    return jnp.dot(left, right, preferred_element_type=jnp.float32)


def kernel(
    fs,
    tp,
    tokens_hbm,
    outer_hbm,
    inner_hbm,
    value_hbm,
    out_hbm,
    up_hbm,
    gate_hbm,
    down_hbm,
    mixer_scales_hbm,
    mixer_taps_hbm,
    out_scale_hbm,
    first_gain_hbm,
    first_shift_hbm,
    up_scales_hbm,
    ffn_taps_hbm,
    ffn_shift_hbm,
    down_scale_hbm,
    second_gain_hbm,
    second_shift_hbm,
    result,
    mix_f,
    out_f,
    up_f,
    gate_f,
    down_f,
    mixer_scales,
    mixer_taps,
    out_scale,
    first_gain,
    first_shift,
    up_scales,
    ffn_taps,
    ffn_shift,
    down_scale,
    second_gain,
    second_shift,
    mix_g,
    out_g,
    ug_g,
    down_g,
    token_all,
    conv_all,
    norm_all,
    guest_all,
    hidden_all,
    hidden_out,
    first_sum,
    total,
    stats,
    load_sem,
    send_sem,
    arrive_sem,
    gather_sem,
    recv_x,
    recv_s,
    recv_g,
    recv_h,
):
    r, z, t = lax.axis_index("rep"), lax.axis_index("fs"), lax.axis_index("tp")
    sibling = t + 1 - 2 * (t % 2)
    across = (t + 2) % tp
    diagonal = (sibling + 2) % tp
    other = 1 - r
    rows, own_width = result.shape
    full_width = own_width * tp
    channels = conv_all.shape[2]
    blocks = ug_g.shape[1]
    last = fs - 1
    own_lanes = pl.ds(pl.multiple_of(t * own_width, own_width), own_width)

    sources = (tokens_hbm, outer_hbm, inner_hbm, value_hbm, out_hbm, up_hbm, gate_hbm, down_hbm)
    sources += (mixer_scales_hbm, mixer_taps_hbm, out_scale_hbm, first_gain_hbm.at[:, own_lanes])
    sources += (first_shift_hbm.at[:, own_lanes], up_scales_hbm, ffn_taps_hbm, ffn_shift_hbm, down_scale_hbm)
    sources += (second_gain_hbm.at[:, own_lanes], second_shift_hbm.at[:, own_lanes])
    places = (token_all.at[t], mix_f.at[0], mix_f.at[1], mix_f.at[2], out_f, up_f, gate_f, down_f)
    places += (mixer_scales, mixer_taps, out_scale, first_gain, first_shift, up_scales, ffn_taps, ffn_shift)
    places += (down_scale, second_gain, second_shift)
    loads = [
        pltpu.make_async_copy(source, place, load_sem.at[number])
        for number, (source, place) in enumerate(zip(sources, places))
    ]
    for load in loads:
        load.start()

    barrier = pltpu.get_barrier_semaphore()
    for peer in (sibling, across, diagonal):
        pl.semaphore_signal(barrier, inc=1, device_id={"tp": peer}, device_id_type=pl.DeviceIdType.MESH)
    pl.semaphore_signal(barrier, inc=1, device_id={"rep": other}, device_id_type=pl.DeviceIdType.MESH)

    @pl.when(z > 0)
    def _():
        pl.semaphore_signal(barrier, inc=1, device_id={"fs": z - 1}, device_id_type=pl.DeviceIdType.MESH)

    @pl.when(z < last)
    def _():
        pl.semaphore_signal(barrier, inc=1, device_id={"fs": z + 1}, device_id_type=pl.DeviceIdType.MESH)

    inside = (z > 0) & (z < last)

    @pl.when(inside)
    def _():
        pl.semaphore_wait(barrier, 6)

    @pl.when(jnp.logical_not(inside))
    def _():
        pl.semaphore_wait(barrier, 5)

    guest_rows = rows // GUEST_PARTS
    return_rows = rows // RETURN_PARTS
    first_hidden, first_guest = 3, 3 + blocks * RETURN_PARTS

    def offset(value, size):
        return value if isinstance(value, int) else pl.multiple_of(value, size)

    def mix_unit(part):
        size = mix_g.shape[1] // (2 * MIX_PARTS)
        return lambda source, half: mix_g.at[source, pl.ds(offset((part * 2 + half) * size, size), size)]

    def out_unit(source, half):
        size = out_g.shape[1] // 2
        return out_g.at[source, pl.ds(offset(half * size, size), size)]

    def ug_unit(block, part):
        size = ug_g.shape[2] // (2 * BLOCK_PARTS[block])
        return lambda source, half: ug_g.at[
            source, block, pl.ds(offset((part * 2 + half) * size, size), size)
        ]

    def down_unit(part):
        size = LANES
        return lambda source, half: down_g.at[source, pl.ds(offset((part * 2 + half) * size, size), size)]

    parts = blocks // 2
    units = [mix_unit(part) for part in range(MIX_PARTS)] + [out_unit]
    out_index, first_down = MIX_PARTS, MIX_PARTS + 1
    units += [down_unit(part) for part in range(parts)]
    first_ug = len(units)
    block_units = []
    for block in range(blocks):
        block_units.append(range(len(units), len(units) + BLOCK_PARTS[block]))
        units += [ug_unit(block, part) for part in range(BLOCK_PARTS[block])]
    count = len(units)

    def program(middle):
        if middle:
            outer, inner, far = (z - 1) * last, last - z, (2 - z) * last
        else:
            near = 1 + z // last
            beyond, far = last - near, last - z
        queues, lowered_blocks = {name: [] for name in LANE_DEPTH}, []
        bases = {}
        for name, depth in LANE_DEPTH.items():
            bases[name] = sum(LANE_DEPTH[other_name] for other_name in bases)

        def send(lane, source, target, recv_sem, device):
            queue, depth = queues[lane], LANE_DEPTH[lane]
            if len(queue) >= depth:
                queue[-depth].wait_send()
            copy = pltpu.make_async_remote_copy(
                src_ref=source,
                dst_ref=target,
                send_sem=send_sem.at[bases[lane] + len(queue) % depth],
                recv_sem=recv_sem,
                device_id=device,
                device_id_type=pl.DeviceIdType.MESH,
            )
            copy.start()
            queue.append(copy)

        def arrived(ref, recv_sem):
            pltpu.make_async_remote_copy(
                src_ref=ref,
                dst_ref=ref,
                send_sem=send_sem.at[0],
                recv_sem=recv_sem,
                device_id={"tp": sibling},
                device_id_type=pl.DeviceIdType.MESH,
            ).wait_recv()

        def moved(number, slot):
            if number < 3:
                return (token_all, conv_all, norm_all)[number].at[slot]
            if number >= first_guest:
                return guest_all.at[slot, pl.ds((number - first_guest) * guest_rows, guest_rows)]
            block, part = (number - first_hidden) // RETURN_PARTS, (number - first_hidden) % RETURN_PARTS
            if middle:
                return hidden_all.at[slot, block]
            return hidden_all.at[slot, block, pl.ds(part * return_rows, return_rows)]

        def exchange_start(number):
            if number == 0:
                loads[0].wait()
            send("x", moved(number, t), moved(number, t), recv_x.at[number, 0], {"tp": across})
            send("d", moved(number, t), moved(number, t), recv_x.at[number, 1], {"tp": sibling})

        def exchange_pass(number):
            arrived(moved(number, across), recv_x.at[number, 0])
            send("d", moved(number, across), moved(number, across), recv_x.at[number, 1], {"tp": sibling})

        def exchange_end(number):
            arrived(moved(number, pl.ds(0, 2)), recv_x.at[number, 1])

        def own(unit):
            ref = units[unit](z, r)
            if middle:
                send("zi", ref, ref, arrive_sem.at[unit, 1], {"fs": inner})
                if unit < first_ug:
                    send("zo", ref, ref, arrive_sem.at[unit, 0], {"fs": outer})
            else:
                send("zi", ref, ref, arrive_sem.at[unit, 0], {"fs": near})

        def own_rest(unit):
            ref = units[unit](z, other)
            send("zi", ref, ref, gather_sem.at[unit], {"fs": near})

        def from_outer(unit):
            ref = units[unit](outer, r)
            arrived(ref, arrive_sem.at[unit, 0])
            send("zi", ref, ref, arrive_sem.at[unit, 2], {"fs": inner})

        def from_inner(unit, source, place):
            ref = units[unit](source, r)
            arrived(ref, arrive_sem.at[unit, place])
            send("y", ref, ref, gather_sem.at[unit], {"rep": other})
            if middle and unit < first_ug:
                send("zo", ref, ref, arrive_sem.at[unit, place], {"fs": outer})

        def need(unit):
            arrived(units[unit](pl.ds(0, 3), 0), gather_sem.at[unit])

        def lower_mix():
            for load in loads[1:4]:
                load.wait()
            for part in range(3):
                mix_g[z, :, part * channels : (part + 1) * channels] = mix_f[part].astype(jnp.bfloat16)

        def lower_out():
            loads[4].wait()
            out_g[z] = out_f[...].astype(jnp.bfloat16)

        def lower_down():
            loads[7].wait()
            down_g[z] = down_f[...].astype(jnp.bfloat16)

        def small_loads():
            for load in loads[8:]:
                load.wait()

        def lower_block(block):
            if not lowered_blocks:
                loads[5].wait()
                loads[6].wait()
            lowered_blocks.append(block)
            columns = slice(block * LANES, (block + 1) * LANES)
            ug_g[z, block, :, :LANES] = up_f[:, columns].astype(jnp.bfloat16)
            ug_g[z, block, :, LANES:] = gate_f[:, columns].astype(jnp.bfloat16)

        def sums_start(number, summed):
            lane = lax.broadcasted_iota(jnp.int32, (rows, LANES), 1)
            one = jnp.sum(summed, axis=1, keepdims=True)
            two = jnp.sum(summed * summed, axis=1, keepdims=True)
            stats[number, t] = jnp.transpose(jnp.where(lane == 0, one, two))[:STAT_ROWS]
            ref = stats.at[number, t]
            for lane_name, peer in (("x", across), ("x", diagonal), ("d", sibling)):
                send(lane_name, ref, ref, recv_s.at[number], {"tp": peer})

        def sums_end(number):
            arrived(stats.at[number, pl.ds(0, 3)], recv_s.at[number])
            summed = stats[number, 0]
            for slot in range(1, tp):
                summed = summed + stats[number, slot]
            back = jnp.transpose(jnp.concatenate([summed] * (LANES // STAT_ROWS), axis=0))
            average = back[:, 0:1] / full_width
            return average, back[:, 1:2] / full_width - average * average

        def mixer():
            for unit in range(MIX_PARTS):
                need(unit)
            exchange_end(0)
            gathered = dot32(token_all[0], mix_g[0])
            for slot in range(1, tp):
                gathered = gathered + dot32(token_all[slot], mix_g[slot])
            scaled = [
                (gathered[:, part * channels : (part + 1) * channels] * mixer_scales[part : part + 1])
                .astype(jnp.bfloat16)
                .astype(jnp.float32)
                for part in range(3)
            ]
            mixed = scaled[0] * shifted_mix(
                scaled[1] * scaled[2], mixer_taps[0:1], mixer_taps[1:2], mixer_taps[2:3]
            )
            conv_all[t] = mixed.astype(jnp.bfloat16)
            exchange_start(1)

        def mixer_output():
            need(out_index)
            exchange_end(1)
            summed = dot32(conv_all[0], out_g[0])
            for slot in range(1, tp):
                summed = summed + dot32(conv_all[slot], out_g[slot])
            summed = summed * out_scale[...] + residual_weight * token_all[t].astype(jnp.float32)
            first_sum[...] = summed
            sums_start(0, summed)

        def first_norm():
            average, spread = sums_end(0)
            norm_all[t] = scaled_norm(
                first_sum[...], average, spread, first_gain[...], first_shift[...]
            ).astype(jnp.bfloat16)

        def guest_send(part):
            lines = pl.ds(part * guest_rows, guest_rows)
            send("zi", norm_all.at[t, lines], guest_all.at[t, lines], recv_g.at[part], {"fs": near})

        def units_of(block, left):
            both = dot32(left(0), ug_g[0, block])
            for slot in range(1, tp):
                both = both + dot32(left(slot), ug_g[slot, block])
            columns = slice(block * LANES, (block + 1) * LANES)
            mixed = []
            for side in range(2):
                mixed.append(
                    shifted_mix(
                        both[:, side * LANES : (side + 1) * LANES] * up_scales[side : side + 1, columns],
                        ffn_taps[0, side : side + 1, columns],
                        ffn_taps[1, side : side + 1, columns],
                        ffn_taps[2, side : side + 1, columns],
                    )
                    + ffn_shift[side : side + 1, columns]
                )
            return (mixed[0] * mixed[1] / (1.0 + jnp.exp(-mixed[1]))).astype(jnp.bfloat16)

        def need_block(block):
            for unit in block_units[block]:
                need(unit)

        def hidden(block):
            hidden_all[t, block] = units_of(block, lambda slot: norm_all[slot])
            exchange_start(first_hidden + block * RETURN_PARTS)

        def give_back(block):
            for part in range(RETURN_PARTS):
                lines = pl.ds(part * return_rows, return_rows)
                number = block * RETURN_PARTS + part
                send(
                    "zo", hidden_out.at[block, lines], hidden_all.at[t, block, lines], recv_h.at[number], {"fs": outer}
                )

        def guest_hidden(block):
            hidden_out[block] = units_of(block, lambda slot: guest_all[slot])
            give_back(block)

        def both_hidden(block):
            units_both = units_of(block, lambda slot: jnp.concatenate([guest_all[slot], norm_all[slot]], axis=0))
            hidden_out[block] = units_both[:rows]
            hidden_all[t, block] = units_both[rows:]
            give_back(block)
            exchange_start(first_hidden + block * RETURN_PARTS)

        def guest_start(part):
            lines = pl.ds(part * guest_rows, guest_rows)
            arrived(guest_all.at[t, lines], recv_g.at[part])
            exchange_start(first_guest + part)

        def returned(number):
            arrived(moved(first_hidden + number, t), recv_h.at[number])
            exchange_start(first_hidden + number)

        def hidden_end(block):
            for part in range(1 if middle else RETURN_PARTS):
                exchange_end(first_hidden + block * RETURN_PARTS + part)

        def down(part):
            need(first_down + part)
            for block in (2 * part, 2 * part + 1):
                hidden_end(block)
            summed = None
            for slot in range(tp):
                left = jnp.concatenate([hidden_all[slot, 2 * part], hidden_all[slot, 2 * part + 1]], axis=1)
                term = dot32(left, down_g[slot, part * 2 * LANES : (part + 1) * 2 * LANES])
                summed = term if summed is None else summed + term
            total[...] = summed if part == 0 else total[...] + summed

        def finish():
            second = total[...] * down_scale[...] + residual_weight * norm_all[t].astype(jnp.float32)
            total[...] = second
            sums_start(1, second)
            average, spread = sums_end(1)
            result[...] = scaled_norm(total[...], average, spread, second_gain[...], second_shift[...]).astype(
                result.dtype
            )
            for name, queue in queues.items():
                for copy in queue[-LANE_DEPTH[name] :]:
                    copy.wait_send()

        if middle:
            lower_mix()
            own(0)
            lower_out()
            own(2)
            own(1)
            exchange_start(0)
            own(3)
            from_outer(0)
            lower_down()
            from_inner(0, inner, 1)
            from_inner(2, inner, 1)
            from_outer(2)
            from_inner(1, inner, 1)
            from_outer(3)
            lower_block(3)
            from_outer(1)
            own(4)
            from_inner(0, far, 2)
            lower_block(5)
            small_loads()
            from_inner(3, inner, 1)
            from_inner(2, far, 2)
            lower_block(1)
            lower_block(0)
            own(9)
            from_inner(3, far, 2)
            from_outer(4)
            lower_block(4)
            from_inner(1, far, 2)
            own(8)
            exchange_pass(0)
            own(5)
            from_inner(4, inner, 1)
            from_inner(9, inner, 1)
            mixer()
            from_inner(4, far, 2)
            from_inner(8, inner, 1)
            own(11)
            own(14)
            from_inner(5, inner, 1)
            own(7)
            exchange_pass(1)
            lower_block(2)
            mixer_output()
            from_inner(11, inner, 1)
            from_outer(9)
            from_inner(14, inner, 1)
            first_norm()
            own(12)
            own(6)
            exchange_start(2)
            from_inner(7, inner, 1)
            from_inner(9, far, 2)
            from_outer(7)
            from_inner(12, inner, 1)
            from_inner(6, inner, 1)
            from_outer(8)
            own(10)
            from_inner(7, far, 2)
            from_outer(10)
            guest_start(0)
            from_outer(6)
            from_outer(5)
            exchange_pass(2)
            from_inner(8, far, 2)
            from_outer(13)
            guest_start(1)
            exchange_end(2)
            from_inner(10, inner, 1)
            from_outer(11)
            exchange_pass(15)
            from_inner(10, far, 2)
            from_inner(6, far, 2)
            exchange_pass(16)
            from_inner(5, far, 2)
            from_outer(12)
            own(13)
            from_inner(13, far, 2)
            need_block(0)
            exchange_end(15)
            exchange_end(16)
            need_block(1)
            both_hidden(1)
            from_inner(11, far, 2)
            from_outer(14)
            both_hidden(0)
            need_block(2)
            from_inner(12, far, 2)
            both_hidden(2)
            from_inner(13, inner, 1)
            need_block(3)
            both_hidden(3)
            from_inner(14, far, 2)
            exchange_pass(5)
            need_block(4)
            both_hidden(4)
            need_block(5)
            both_hidden(5)
            exchange_pass(11)
            exchange_pass(7)
            exchange_pass(3)
            exchange_pass(9)
            exchange_pass(13)
            down(0)
            down(1)
            down(2)
            finish()
        else:
            lower_mix()
            own(0)
            lower_out()
            own(3)
            own(2)
            own(1)
            own(4)
            lower_down()
            lower_block(3)
            own_rest(3)
            exchange_start(0)
            small_loads()
            from_inner(0, near, 0)
            own_rest(1)
            from_inner(2, near, 0)
            from_inner(3, near, 0)
            own_rest(2)
            lower_block(1)
            own_rest(0)
            from_inner(0, beyond, 1)
            lower_block(2)
            own(5)
            from_inner(2, beyond, 1)
            own(10)
            from_inner(1, beyond, 1)
            lower_block(5)
            from_inner(1, near, 0)
            own(9)
            from_inner(0, far, 2)
            from_inner(3, beyond, 1)
            own_rest(4)
            lower_block(0)
            from_inner(2, far, 2)
            own(6)
            from_inner(3, far, 2)
            exchange_pass(0)
            from_inner(1, far, 2)
            own(11)
            mixer()
            from_inner(4, near, 0)
            from_inner(4, beyond, 1)
            from_inner(4, far, 2)
            own(13)
            own(7)
            exchange_pass(1)
            lower_block(4)
            own(8)
            mixer_output()
            first_norm()
            guest_send(0)
            guest_send(1)
            from_inner(5, beyond, 1)
            from_inner(5, near, 0)
            own_rest(9)
            own(14)
            from_inner(6, near, 0)
            own(12)
            from_inner(7, beyond, 1)
            own_rest(8)
            from_inner(7, far, 2)
            own_rest(11)
            own_rest(10)
            from_inner(7, near, 0)
            own_rest(14)
            own_rest(12)
            returned(2)
            from_inner(5, far, 2)
            returned(3)
            own_rest(13)
            returned(0)
            returned(1)
            exchange_pass(6)
            from_inner(6, beyond, 1)
            returned(4)
            own_rest(6)
            returned(5)
            returned(6)
            exchange_pass(5)
            own_rest(5)
            from_inner(6, far, 2)
            exchange_pass(4)
            own_rest(7)
            returned(7)
            returned(8)
            returned(9)
            exchange_pass(3)
            returned(10)
            exchange_pass(10)
            exchange_pass(8)
            exchange_pass(7)
            exchange_pass(11)
            returned(11)
            exchange_pass(9)
            exchange_pass(12)
            exchange_pass(13)
            down(0)
            exchange_pass(14)
            down(1)
            down(2)
            finish()
    @pl.when(inside)
    def _():
        program(True)

    @pl.when(jnp.logical_not(inside))
    def _():
        program(False)


def fused(
    fs,
    tp,
    tokens,
    outer_gate,
    inner_gate,
    mixer_value,
    mixer_scales,
    mixer_taps,
    mixer_out,
    out_scale,
    first_gain,
    first_shift,
    up_proj,
    gate_proj,
    up_scales,
    ffn_taps,
    ffn_shift,
    down_proj,
    down_scale,
    second_gain,
    second_shift,
):
    rows, own_width = tokens.shape
    depth, channels = outer_gate.shape
    hidden = up_proj.shape[1]
    blocks = hidden // LANES
    count = MIX_PARTS + 1 + blocks // 2 + sum(BLOCK_PARTS)
    moves = 3 + blocks * RETURN_PARTS + GUEST_PARTS
    any_space = pl.BlockSpec(memory_space=pl.ANY)
    in_vmem = pl.BlockSpec(memory_space=pltpu.VMEM)

    def row(vector):
        return vector.reshape(1, -1)

    return pl.pallas_call(
        functools.partial(kernel, fs, tp),
        out_shape=jax.ShapeDtypeStruct((rows, own_width), jnp.bfloat16),
        in_specs=[any_space] * 19,
        out_specs=in_vmem,
        scratch_shapes=[
            pltpu.VMEM((3, depth, channels), jnp.float32),
            pltpu.VMEM(mixer_out.shape, jnp.float32),
            pltpu.VMEM(up_proj.shape, jnp.float32),
            pltpu.VMEM(gate_proj.shape, jnp.float32),
            pltpu.VMEM(down_proj.shape, jnp.float32),
            pltpu.VMEM(mixer_scales.shape, jnp.float32),
            pltpu.VMEM(mixer_taps.shape, jnp.float32),
            pltpu.VMEM((1, own_width), jnp.float32),
            pltpu.VMEM((1, own_width), jnp.float32),
            pltpu.VMEM((1, own_width), jnp.float32),
            pltpu.VMEM(up_scales.shape, jnp.float32),
            pltpu.VMEM(ffn_taps.shape, jnp.float32),
            pltpu.VMEM(ffn_shift.shape, jnp.float32),
            pltpu.VMEM((1, own_width), jnp.float32),
            pltpu.VMEM((1, own_width), jnp.float32),
            pltpu.VMEM((1, own_width), jnp.float32),
            pltpu.VMEM((fs, depth, 3 * channels), jnp.bfloat16),
            pltpu.VMEM((fs,) + mixer_out.shape, jnp.bfloat16),
            pltpu.VMEM((fs, blocks, depth, 2 * LANES), jnp.bfloat16),
            pltpu.VMEM((fs,) + down_proj.shape, jnp.bfloat16),
            pltpu.VMEM((tp, rows, own_width), jnp.bfloat16),
            pltpu.VMEM((tp, rows, channels), jnp.bfloat16),
            pltpu.VMEM((tp, rows, own_width), jnp.bfloat16),
            pltpu.VMEM((tp, rows, own_width), jnp.bfloat16),
            pltpu.VMEM((tp, blocks, rows, LANES), jnp.bfloat16),
            pltpu.VMEM((blocks, rows, LANES), jnp.bfloat16),
            pltpu.VMEM((rows, own_width), jnp.float32),
            pltpu.VMEM((rows, own_width), jnp.float32),
            pltpu.VMEM((2, tp, STAT_ROWS, rows), jnp.float32),
            pltpu.SemaphoreType.DMA((19,)),
            pltpu.SemaphoreType.DMA((sum(LANE_DEPTH.values()),)),
            pltpu.SemaphoreType.DMA((count, 3)),
            pltpu.SemaphoreType.DMA((count,)),
            pltpu.SemaphoreType.DMA((moves, 2)),
            pltpu.SemaphoreType.DMA((2,)),
            pltpu.SemaphoreType.DMA((GUEST_PARTS,)),
            pltpu.SemaphoreType.DMA((blocks * RETURN_PARTS,)),
        ],
        compiler_params=pltpu.CompilerParams(
            collective_id=0, has_side_effects=True, vmem_limit_bytes=60 * 1024 * 1024
        ),
    )(
        tokens,
        outer_gate,
        inner_gate,
        mixer_value,
        mixer_out,
        up_proj,
        gate_proj,
        down_proj,
        mixer_scales,
        mixer_taps,
        row(out_scale),
        row(first_gain),
        row(first_shift),
        up_scales,
        ffn_taps,
        ffn_shift,
        row(down_scale),
        row(second_gain),
        row(second_shift),
    )


def fits(mesh):
    return mesh.shape["rep"] == 2 and mesh.shape["fs"] == 4 and mesh.shape["tp"] == 4


def solution(mesh):
    body = functools.partial(fused, mesh.shape["fs"], mesh.shape["tp"]) if fits(mesh) else local
    return jax.shard_map(
        body,
        mesh=mesh,
        in_specs=(
            P(("rep", "fs"), "tp"),
            P("fs", "tp"),
            P("fs", "tp"),
            P("fs", "tp"),
            P(None, "tp"),
            P(None, "tp"),
            P("fs", "tp"),
            P("tp"),
            P(),
            P(),
            P("fs", "tp"),
            P("fs", "tp"),
            P(None, "tp"),
            P(None, None, "tp"),
            P(None, "tp"),
            P("fs", "tp"),
            P("tp"),
            P(),
            P(),
        ),
        out_specs=P(("rep", "fs"), "tp"),
        check_vma=False,
    )
```

```python
import functools

import jax
import jax.numpy as jnp
from jax import lax
from jax.experimental import pallas as pl
from jax.experimental.pallas import tpu as pltpu
from jax.sharding import PartitionSpec as P

LEN = 128


norm_eps = 1e-05
residual_weight = 8.0**0.25


def causal_mix(signal, kernel_taps):
    sequences = signal.reshape(-1, LEN, signal.shape[-1])
    padded = jnp.pad(sequences, ((0, 0), (2, 0), (0, 0)))
    mixed = (
        kernel_taps[0] * padded[:, :-2]
        + kernel_taps[1] * padded[:, 1:-1]
        + kernel_taps[2] * padded[:, 2:]
    )
    return mixed.reshape(signal.shape)


def lowered(matrix):
    return matrix.astype(jnp.bfloat16)


def single_fold(operand, portion):
    return jnp.dot(operand, portion, preferred_element_type=jnp.float32)


def fold_step(operand, pieces):
    result = []
    for number in range(len(pieces)):
        result.append(jnp.dot(operand, pieces[number], preferred_element_type=jnp.float32))
    return tuple(result)


def own_columns(vector, own_width):
    return lax.dynamic_slice_in_dim(vector, lax.axis_index("tp") * own_width, own_width, 0)


def scaled_norm(summed, average, spread, gain_vector, shift_vector):
    return (summed - average) * lax.rsqrt(spread + norm_eps) * gain_vector + shift_vector


def local(
    tokens,
    outer_gate,
    inner_gate,
    mixer_value,
    mixer_scales,
    mixer_taps,
    mixer_out,
    out_scale,
    first_gain,
    first_shift,
    up_proj,
    gate_proj,
    up_scales,
    ffn_taps,
    ffn_shift,
    down_proj,
    down_scale,
    second_gain,
    second_shift,
):
    own_width = tokens.shape[1]
    full_width = own_width * lax.axis_size("tp")
    token_whole = lax.all_gather(tokens, "tp", axis=1, tiled=True)
    outer_part, inner_part, value_part = fold_step(
        token_whole,
        (
            lax.all_gather(lowered(outer_gate), "fs", axis=0, tiled=True),
            lax.all_gather(lowered(inner_gate), "fs", axis=0, tiled=True),
            lax.all_gather(lowered(mixer_value), "fs", axis=0, tiled=True),
        ),
    )
    outer_part = (outer_part * mixer_scales[0]).astype(jnp.bfloat16)
    inner_part = (inner_part * mixer_scales[1]).astype(jnp.bfloat16)
    value_part = (value_part * mixer_scales[2]).astype(jnp.bfloat16)
    product = inner_part.astype(jnp.float32) * value_part.astype(jnp.float32)
    mixed_conv = (outer_part.astype(jnp.float32) * causal_mix(product, mixer_taps)).astype(
        jnp.bfloat16
    )
    conv_whole = lax.all_gather(mixed_conv, "tp", axis=1, tiled=True)
    mixer_sum = (
        single_fold(conv_whole, lax.all_gather(lowered(mixer_out), "fs", axis=0, tiled=True))
        * out_scale
    )
    first_sum = residual_weight * tokens.astype(jnp.float32) + mixer_sum
    row_total, row_square = lax.psum(
        (jnp.sum(first_sum, 1, keepdims=True), jnp.sum(first_sum * first_sum, 1, keepdims=True)),
        "tp",
    )
    average = row_total / full_width
    spread = row_square / full_width - average * average
    normed = scaled_norm(
        first_sum,
        average,
        spread,
        own_columns(first_gain, own_width),
        own_columns(first_shift, own_width),
    ).astype(jnp.bfloat16)
    normed_whole = lax.all_gather(normed, "tp", axis=1, tiled=True)
    up_matrix, gate_matrix = (
        lax.all_gather(lowered(up_proj), "fs", axis=0, tiled=True),
        lax.all_gather(lowered(gate_proj), "fs", axis=0, tiled=True),
    )
    up_linear = jnp.dot(normed_whole, up_matrix, preferred_element_type=jnp.float32)
    gate_linear = jnp.dot(normed_whole, gate_matrix, preferred_element_type=jnp.float32)
    up_linear = up_linear * up_scales[0]
    gate_linear = gate_linear * up_scales[1]
    up_mixed = causal_mix(up_linear, ffn_taps[:, 0]) + ffn_shift[0]
    gate_mixed = causal_mix(gate_linear, ffn_taps[:, 1]) + ffn_shift[1]
    hidden = (up_mixed * jax.nn.silu(gate_mixed)).astype(jnp.bfloat16)
    hidden_whole = lax.all_gather(hidden, "tp", axis=1, tiled=True)
    ffn_sum = (
        single_fold(hidden_whole, lax.all_gather(lowered(down_proj), "fs", axis=0, tiled=True))
        * down_scale
    )
    second_sum = residual_weight * normed.astype(jnp.float32) + ffn_sum
    second_total, second_square = lax.psum(
        (jnp.sum(second_sum, 1, keepdims=True), jnp.sum(second_sum * second_sum, 1, keepdims=True)),
        "tp",
    )
    second_average = second_total / full_width
    second_spread = second_square / full_width - second_average * second_average
    return scaled_norm(
        second_sum,
        second_average,
        second_spread,
        own_columns(second_gain, own_width),
        own_columns(second_shift, own_width),
    ).astype(jnp.bfloat16)


LANES = 128
STAT_ROWS = 2
GUEST_PARTS = 2
ROW_CUT = 128
RETURN_PARTS = 2
MIX_PARTS = 4
BLOCK_PARTS = (1, 1, 1, 1, 1, 2)
LANE_DEPTH = {"zi": 14, "zo": 8, "y": 8, "x": 8, "d": 8}


def shifted_mix(signal, first, second, third):
    rows = lax.broadcasted_iota(jnp.int32, signal.shape, 0) % LEN
    one = jnp.where(rows >= 1, pltpu.roll(signal, 1, 0), 0.0)
    two = jnp.where(rows >= 2, pltpu.roll(signal, 2, 0), 0.0)
    return first * two + second * one + third * signal


def dot32(left, right):
    return jnp.dot(left, right, preferred_element_type=jnp.float32)


def kernel(
    fs,
    tp,
    tokens_hbm,
    outer_hbm,
    inner_hbm,
    value_hbm,
    out_hbm,
    up_hbm,
    gate_hbm,
    down_hbm,
    mixer_scales_hbm,
    mixer_taps_hbm,
    out_scale_hbm,
    first_gain_hbm,
    first_shift_hbm,
    up_scales_hbm,
    ffn_taps_hbm,
    ffn_shift_hbm,
    down_scale_hbm,
    second_gain_hbm,
    second_shift_hbm,
    result,
    mix_f,
    out_f,
    up_f,
    gate_f,
    down_f,
    mixer_scales,
    mixer_taps,
    out_scale,
    first_gain,
    first_shift,
    up_scales,
    ffn_taps,
    ffn_shift,
    down_scale,
    second_gain,
    second_shift,
    mix_g,
    out_g,
    ug_g,
    down_g,
    token_all,
    conv_all,
    norm_all,
    guest_all,
    hidden_all,
    hidden_out,
    first_sum,
    total,
    stats,
    load_sem,
    send_sem,
    arrive_sem,
    gather_sem,
    recv_x,
    recv_s,
    recv_g,
    recv_h,
):
    r, z, t = lax.axis_index("rep"), lax.axis_index("fs"), lax.axis_index("tp")
    sibling = t + 1 - 2 * (t % 2)
    across = (t + 2) % tp
    diagonal = (sibling + 2) % tp
    other = 1 - r
    rows, own_width = result.shape
    full_width = own_width * tp
    channels = conv_all.shape[2]
    blocks = ug_g.shape[1]
    last = fs - 1
    own_lanes = pl.ds(pl.multiple_of(t * own_width, own_width), own_width)

    sources = (tokens_hbm, outer_hbm, inner_hbm, value_hbm, out_hbm, up_hbm, gate_hbm, down_hbm)
    sources += (mixer_scales_hbm, mixer_taps_hbm, out_scale_hbm, first_gain_hbm.at[:, own_lanes])
    sources += (first_shift_hbm.at[:, own_lanes], up_scales_hbm, ffn_taps_hbm, ffn_shift_hbm, down_scale_hbm)
    sources += (second_gain_hbm.at[:, own_lanes], second_shift_hbm.at[:, own_lanes])
    places = (token_all.at[t], mix_f.at[0], mix_f.at[1], mix_f.at[2], out_f, up_f, gate_f, down_f)
    places += (mixer_scales, mixer_taps, out_scale, first_gain, first_shift, up_scales, ffn_taps, ffn_shift)
    places += (down_scale, second_gain, second_shift)
    loads = [
        pltpu.make_async_copy(source, place, load_sem.at[number])
        for number, (source, place) in enumerate(zip(sources, places))
    ]
    for load in loads:
        load.start()

    barrier = pltpu.get_barrier_semaphore()
    for peer in (sibling, across, diagonal):
        pl.semaphore_signal(barrier, inc=1, device_id={"tp": peer}, device_id_type=pl.DeviceIdType.MESH)
    pl.semaphore_signal(barrier, inc=1, device_id={"rep": other}, device_id_type=pl.DeviceIdType.MESH)

    @pl.when(z > 0)
    def _():
        pl.semaphore_signal(barrier, inc=1, device_id={"fs": z - 1}, device_id_type=pl.DeviceIdType.MESH)

    @pl.when(z < last)
    def _():
        pl.semaphore_signal(barrier, inc=1, device_id={"fs": z + 1}, device_id_type=pl.DeviceIdType.MESH)

    inside = (z > 0) & (z < last)

    @pl.when(inside)
    def _():
        pl.semaphore_wait(barrier, 6)

    @pl.when(jnp.logical_not(inside))
    def _():
        pl.semaphore_wait(barrier, 5)

    guest_rows = rows // GUEST_PARTS
    return_rows = rows // RETURN_PARTS
    first_hidden, first_guest = 3, 3 + blocks * RETURN_PARTS

    def offset(value, size):
        return value if isinstance(value, int) else pl.multiple_of(value, size)

    def mix_unit(part):
        size = mix_g.shape[1] // (2 * MIX_PARTS)
        return lambda source, half: mix_g.at[source, pl.ds(offset((part * 2 + half) * size, size), size)]

    def out_unit(source, half):
        size = out_g.shape[1] // 2
        return out_g.at[source, pl.ds(offset(half * size, size), size)]

    def ug_unit(block, part):
        size = ug_g.shape[2] // (2 * BLOCK_PARTS[block])
        return lambda source, half: ug_g.at[
            source, block, pl.ds(offset((part * 2 + half) * size, size), size)
        ]

    def down_unit(part):
        size = LANES
        return lambda source, half: down_g.at[source, pl.ds(offset((part * 2 + half) * size, size), size)]

    parts = blocks // 2
    units = [mix_unit(part) for part in range(MIX_PARTS)] + [out_unit]
    out_index, first_down = MIX_PARTS, MIX_PARTS + 1
    units += [down_unit(part) for part in range(parts)]
    first_ug = len(units)
    block_units = []
    for block in range(blocks):
        block_units.append(range(len(units), len(units) + BLOCK_PARTS[block]))
        units += [ug_unit(block, part) for part in range(BLOCK_PARTS[block])]
    count = len(units)

    def program(middle):
        if middle:
            outer, inner, far = (z - 1) * last, last - z, (2 - z) * last
        else:
            near = 1 + z // last
            beyond, far = last - near, last - z
        queues, lowered_blocks = {name: [] for name in LANE_DEPTH}, []
        bases = {}
        for name, depth in LANE_DEPTH.items():
            bases[name] = sum(LANE_DEPTH[other_name] for other_name in bases)

        def send(lane, source, target, recv_sem, device):
            queue, depth = queues[lane], LANE_DEPTH[lane]
            if len(queue) >= depth:
                queue[-depth].wait_send()
            copy = pltpu.make_async_remote_copy(
                src_ref=source,
                dst_ref=target,
                send_sem=send_sem.at[bases[lane] + len(queue) % depth],
                recv_sem=recv_sem,
                device_id=device,
                device_id_type=pl.DeviceIdType.MESH,
            )
            copy.start()
            queue.append(copy)

        def arrived(ref, recv_sem):
            pltpu.make_async_remote_copy(
                src_ref=ref,
                dst_ref=ref,
                send_sem=send_sem.at[0],
                recv_sem=recv_sem,
                device_id={"tp": sibling},
                device_id_type=pl.DeviceIdType.MESH,
            ).wait_recv()

        def moved(number, slot):
            if number < 3:
                return (token_all, conv_all, norm_all)[number].at[slot]
            if number >= first_guest:
                return guest_all.at[slot, pl.ds((number - first_guest) * guest_rows, guest_rows)]
            block, part = (number - first_hidden) // RETURN_PARTS, (number - first_hidden) % RETURN_PARTS
            if middle:
                return hidden_all.at[slot, block]
            return hidden_all.at[slot, block, pl.ds(part * return_rows, return_rows)]

        def exchange_start(number):
            if number == 0:
                loads[0].wait()
            send("x", moved(number, t), moved(number, t), recv_x.at[number, 0], {"tp": across})
            send("d", moved(number, t), moved(number, t), recv_x.at[number, 1], {"tp": sibling})

        def exchange_pass(number):
            arrived(moved(number, across), recv_x.at[number, 0])
            send("d", moved(number, across), moved(number, across), recv_x.at[number, 1], {"tp": sibling})

        def exchange_end(number):
            arrived(moved(number, pl.ds(0, 2)), recv_x.at[number, 1])

        def own(unit):
            ref = units[unit](z, r)
            if middle:
                send("zi", ref, ref, arrive_sem.at[unit, 1], {"fs": inner})
                if unit < first_ug:
                    send("zo", ref, ref, arrive_sem.at[unit, 0], {"fs": outer})
            else:
                send("zi", ref, ref, arrive_sem.at[unit, 0], {"fs": near})

        def own_rest(unit):
            ref = units[unit](z, other)
            send("zi", ref, ref, gather_sem.at[unit], {"fs": near})

        def from_outer(unit):
            ref = units[unit](outer, r)
            arrived(ref, arrive_sem.at[unit, 0])
            send("zi", ref, ref, arrive_sem.at[unit, 2], {"fs": inner})

        def from_inner(unit, source, place):
            ref = units[unit](source, r)
            arrived(ref, arrive_sem.at[unit, place])
            send("y", ref, ref, gather_sem.at[unit], {"rep": other})
            if middle and unit < first_ug:
                send("zo", ref, ref, arrive_sem.at[unit, place], {"fs": outer})

        def need(unit):
            arrived(units[unit](pl.ds(0, 3), 0), gather_sem.at[unit])

        def lower_mix():
            for load in loads[1:4]:
                load.wait()
            for part in range(3):
                mix_g[z, :, part * channels : (part + 1) * channels] = mix_f[part].astype(jnp.bfloat16)

        def lower_out():
            loads[4].wait()
            out_g[z] = out_f[...].astype(jnp.bfloat16)

        def lower_down():
            loads[7].wait()
            down_g[z] = down_f[...].astype(jnp.bfloat16)

        def small_loads():
            for load in loads[8:]:
                load.wait()

        def lower_block(block):
            if not lowered_blocks:
                loads[5].wait()
                loads[6].wait()
            lowered_blocks.append(block)
            columns = slice(block * LANES, (block + 1) * LANES)
            ug_g[z, block, :, :LANES] = up_f[:, columns].astype(jnp.bfloat16)
            ug_g[z, block, :, LANES:] = gate_f[:, columns].astype(jnp.bfloat16)

        def sums_start(number, summed):
            lane = lax.broadcasted_iota(jnp.int32, (rows, LANES), 1)
            one = jnp.sum(summed, axis=1, keepdims=True)
            two = jnp.sum(summed * summed, axis=1, keepdims=True)
            stats[number, t] = jnp.transpose(jnp.where(lane == 0, one, two))[:STAT_ROWS]
            ref = stats.at[number, t]
            for lane_name, peer in (("x", across), ("x", diagonal), ("d", sibling)):
                send(lane_name, ref, ref, recv_s.at[number], {"tp": peer})

        def sums_end(number):
            arrived(stats.at[number, pl.ds(0, 3)], recv_s.at[number])
            summed = stats[number, 0]
            for slot in range(1, tp):
                summed = summed + stats[number, slot]
            back = jnp.transpose(jnp.concatenate([summed] * (LANES // STAT_ROWS), axis=0))
            average = back[:, 0:1] / full_width
            return average, back[:, 1:2] / full_width - average * average

        def mixer():
            for unit in range(MIX_PARTS):
                need(unit)
            exchange_end(0)
            gathered = dot32(token_all[0], mix_g[0])
            for slot in range(1, tp):
                gathered = gathered + dot32(token_all[slot], mix_g[slot])
            scaled = [
                (gathered[:, part * channels : (part + 1) * channels] * mixer_scales[part : part + 1])
                .astype(jnp.bfloat16)
                .astype(jnp.float32)
                for part in range(3)
            ]
            mixed = scaled[0] * shifted_mix(
                scaled[1] * scaled[2], mixer_taps[0:1], mixer_taps[1:2], mixer_taps[2:3]
            )
            conv_all[t] = mixed.astype(jnp.bfloat16)
            exchange_start(1)

        def mixer_output():
            need(out_index)
            exchange_end(1)
            summed = dot32(conv_all[0], out_g[0])
            for slot in range(1, tp):
                summed = summed + dot32(conv_all[slot], out_g[slot])
            summed = summed * out_scale[...] + residual_weight * token_all[t].astype(jnp.float32)
            first_sum[...] = summed
            sums_start(0, summed)

        def first_norm():
            average, spread = sums_end(0)
            norm_all[t] = scaled_norm(
                first_sum[...], average, spread, first_gain[...], first_shift[...]
            ).astype(jnp.bfloat16)

        def guest_send(part):
            lines = pl.ds(part * guest_rows, guest_rows)
            send("zi", norm_all.at[t, lines], guest_all.at[t, lines], recv_g.at[part], {"fs": near})

        def units_of(block, left, lines):
            both = dot32(left(0, lines), ug_g[0, block])
            for slot in range(1, tp):
                both = both + dot32(left(slot, lines), ug_g[slot, block])
            columns = slice(block * LANES, (block + 1) * LANES)
            mixed = []
            for side in range(2):
                mixed.append(
                    shifted_mix(
                        both[:, side * LANES : (side + 1) * LANES] * up_scales[side : side + 1, columns],
                        ffn_taps[0, side : side + 1, columns],
                        ffn_taps[1, side : side + 1, columns],
                        ffn_taps[2, side : side + 1, columns],
                    )
                    + ffn_shift[side : side + 1, columns]
                )
            return (mixed[0] * mixed[1] / (1.0 + jnp.exp(-mixed[1]))).astype(jnp.bfloat16)

        row_cuts = [slice(first, first + ROW_CUT) for first in range(0, rows, ROW_CUT)]

        def store_units(block, left, target):
            for lines in row_cuts:
                target[lines] = units_of(block, lambda slot, lines: left[slot, lines], lines)

        def need_block(block):
            for unit in block_units[block]:
                need(unit)

        def hidden(block):
            store_units(block, norm_all, hidden_all.at[t, block])
            exchange_start(first_hidden + block * RETURN_PARTS)

        def give_back(block):
            for part in range(RETURN_PARTS):
                lines = pl.ds(part * return_rows, return_rows)
                number = block * RETURN_PARTS + part
                send(
                    "zo", hidden_out.at[block, lines], hidden_all.at[t, block, lines], recv_h.at[number], {"fs": outer}
                )

        def guest_hidden(block):
            store_units(block, guest_all, hidden_out.at[block])
            give_back(block)

        def both_hidden(block):
            store_units(block, guest_all, hidden_out.at[block])
            store_units(block, norm_all, hidden_all.at[t, block])
            give_back(block)
            exchange_start(first_hidden + block * RETURN_PARTS)

        def guest_start(part):
            lines = pl.ds(part * guest_rows, guest_rows)
            arrived(guest_all.at[t, lines], recv_g.at[part])
            exchange_start(first_guest + part)

        def returned(number):
            arrived(moved(first_hidden + number, t), recv_h.at[number])
            exchange_start(first_hidden + number)

        def hidden_end(block):
            for part in range(1 if middle else RETURN_PARTS):
                exchange_end(first_hidden + block * RETURN_PARTS + part)

        def down(part):
            need(first_down + part)
            for block in (2 * part, 2 * part + 1):
                hidden_end(block)
            summed = None
            for slot in range(tp):
                left = jnp.concatenate([hidden_all[slot, 2 * part], hidden_all[slot, 2 * part + 1]], axis=1)
                term = dot32(left, down_g[slot, part * 2 * LANES : (part + 1) * 2 * LANES])
                summed = term if summed is None else summed + term
            total[...] = summed if part == 0 else total[...] + summed

        def finish():
            second = total[...] * down_scale[...] + residual_weight * norm_all[t].astype(jnp.float32)
            total[...] = second
            sums_start(1, second)
            average, spread = sums_end(1)
            result[...] = scaled_norm(total[...], average, spread, second_gain[...], second_shift[...]).astype(
                result.dtype
            )
            for name, queue in queues.items():
                for copy in queue[-LANE_DEPTH[name] :]:
                    copy.wait_send()

        if middle:
            lower_mix()
            own(3)
            own(0)
            own(1)
            own(2)
            exchange_start(0)
            from_inner(3, inner, 1)
            from_outer(2)
            from_outer(1)
            from_inner(0, inner, 1)
            from_outer(0)
            from_inner(1, inner, 1)
            lower_out()
            from_outer(3)
            from_inner(2, inner, 1)
            from_outer(4)
            lower_down()
            own(4)
            from_inner(2, far, 2)
            lower_block(3)
            from_inner(0, far, 2)
            from_inner(1, far, 2)
            lower_block(1)
            from_inner(3, far, 2)
            own(9)
            exchange_pass(0)
            small_loads()
            lower_block(4)
            own(11)
            from_inner(4, inner, 1)
            lower_block(2)
            from_inner(4, far, 2)
            own(5)
            lower_block(0)
            from_inner(9, inner, 1)
            mixer()
            own(12)
            own(8)
            from_inner(11, inner, 1)
            exchange_pass(1)
            from_outer(9)
            from_inner(5, inner, 1)
            from_outer(7)
            own(6)
            from_inner(12, inner, 1)
            mixer_output()
            from_inner(8, inner, 1)
            first_norm()
            own(10)
            from_outer(8)
            exchange_start(2)
            from_inner(7, far, 2)
            lower_block(5)
            from_inner(9, far, 2)
            from_outer(6)
            from_inner(6, inner, 1)
            own(7)
            from_outer(10)
            from_outer(5)
            from_inner(10, inner, 1)
            guest_start(0)
            from_inner(6, far, 2)
            from_inner(8, far, 2)
            from_inner(7, inner, 1)
            exchange_pass(2)
            from_outer(11)
            guest_start(1)
            exchange_pass(15)
            need_block(1)
            need_block(0)
            exchange_end(2)
            from_inner(10, far, 2)
            exchange_end(15)
            own(13)
            from_inner(5, far, 2)
            hidden(0)
            from_outer(12)
            exchange_pass(16)
            hidden(1)
            from_outer(13)
            own(14)
            exchange_end(16)
            from_inner(11, far, 2)
            guest_hidden(1)
            guest_hidden(0)
            from_inner(12, far, 2)
            from_outer(14)
            need_block(2)
            guest_hidden(2)
            from_inner(13, inner, 1)
            from_inner(13, far, 2)
            from_inner(14, inner, 1)
            need_block(3)
            hidden(3)
            guest_hidden(3)
            from_inner(14, far, 2)
            hidden(2)
            need_block(4)
            guest_hidden(4)
            hidden(4)
            need_block(5)
            guest_hidden(5)
            exchange_pass(7)
            hidden(5)
            exchange_pass(3)
            exchange_pass(5)
            down(0)
            exchange_pass(9)
            exchange_pass(11)
            exchange_pass(13)
            down(1)
            down(2)
            finish()
        else:
            lower_mix()
            own(2)
            own(1)
            own(0)
            lower_out()
            lower_down()
            own(3)
            lower_block(1)
            exchange_start(0)
            own(4)
            from_inner(0, near, 0)
            own_rest(3)
            from_inner(3, near, 0)
            own_rest(0)
            lower_block(5)
            own_rest(1)
            own_rest(2)
            from_inner(3, beyond, 1)
            from_inner(2, near, 0)
            lower_block(4)
            own(5)
            from_inner(0, beyond, 1)
            from_inner(1, near, 0)
            from_inner(1, beyond, 1)
            from_inner(2, far, 2)
            lower_block(2)
            own_rest(4)
            lower_block(0)
            own(8)
            own(9)
            from_inner(2, beyond, 1)
            exchange_pass(0)
            from_inner(1, far, 2)
            lower_block(3)
            from_inner(3, far, 2)
            own(7)
            from_inner(0, far, 2)
            own_rest(8)
            small_loads()
            own(6)
            own(10)
            from_inner(4, far, 2)
            from_inner(4, beyond, 1)
            mixer()
            from_inner(4, near, 0)
            own(11)
            exchange_pass(1)
            mixer_output()
            first_norm()
            guest_send(0)
            from_inner(7, far, 2)
            from_inner(5, near, 0)
            guest_send(1)
            own_rest(9)
            own(12)
            own(13)
            own_rest(10)
            own(14)
            own_rest(11)
            from_inner(6, far, 2)
            own_rest(12)
            returned(2)
            own_rest(14)
            returned(3)
            from_inner(6, near, 0)
            own_rest(13)
            from_inner(7, beyond, 1)
            returned(0)
            from_inner(5, far, 2)
            returned(1)
            own_rest(6)
            own_rest(5)
            own_rest(7)
            from_inner(6, beyond, 1)
            returned(4)
            returned(5)
            exchange_pass(4)
            returned(6)
            returned(7)
            returned(8)
            exchange_pass(6)
            exchange_pass(8)
            exchange_pass(5)
            returned(9)
            from_inner(5, beyond, 1)
            exchange_pass(10)
            exchange_pass(9)
            returned(10)
            exchange_pass(7)
            from_inner(7, near, 0)
            exchange_pass(3)
            returned(11)
            exchange_pass(11)
            down(0)
            exchange_pass(13)
            exchange_pass(12)
            exchange_pass(14)
            down(1)
            down(2)
            finish()
    @pl.when(inside)
    def _():
        program(True)

    @pl.when(jnp.logical_not(inside))
    def _():
        program(False)


def fused(
    fs,
    tp,
    tokens,
    outer_gate,
    inner_gate,
    mixer_value,
    mixer_scales,
    mixer_taps,
    mixer_out,
    out_scale,
    first_gain,
    first_shift,
    up_proj,
    gate_proj,
    up_scales,
    ffn_taps,
    ffn_shift,
    down_proj,
    down_scale,
    second_gain,
    second_shift,
):
    rows, own_width = tokens.shape
    depth, channels = outer_gate.shape
    hidden = up_proj.shape[1]
    blocks = hidden // LANES
    count = MIX_PARTS + 1 + blocks // 2 + sum(BLOCK_PARTS)
    moves = 3 + blocks * RETURN_PARTS + GUEST_PARTS
    any_space = pl.BlockSpec(memory_space=pl.ANY)
    in_vmem = pl.BlockSpec(memory_space=pltpu.VMEM)

    def row(vector):
        return vector.reshape(1, -1)

    return pl.pallas_call(
        functools.partial(kernel, fs, tp),
        out_shape=jax.ShapeDtypeStruct((rows, own_width), jnp.bfloat16),
        in_specs=[any_space] * 19,
        out_specs=in_vmem,
        scratch_shapes=[
            pltpu.VMEM((3, depth, channels), jnp.float32),
            pltpu.VMEM(mixer_out.shape, jnp.float32),
            pltpu.VMEM(up_proj.shape, jnp.float32),
            pltpu.VMEM(gate_proj.shape, jnp.float32),
            pltpu.VMEM(down_proj.shape, jnp.float32),
            pltpu.VMEM(mixer_scales.shape, jnp.float32),
            pltpu.VMEM(mixer_taps.shape, jnp.float32),
            pltpu.VMEM((1, own_width), jnp.float32),
            pltpu.VMEM((1, own_width), jnp.float32),
            pltpu.VMEM((1, own_width), jnp.float32),
            pltpu.VMEM(up_scales.shape, jnp.float32),
            pltpu.VMEM(ffn_taps.shape, jnp.float32),
            pltpu.VMEM(ffn_shift.shape, jnp.float32),
            pltpu.VMEM((1, own_width), jnp.float32),
            pltpu.VMEM((1, own_width), jnp.float32),
            pltpu.VMEM((1, own_width), jnp.float32),
            pltpu.VMEM((fs, depth, 3 * channels), jnp.bfloat16),
            pltpu.VMEM((fs,) + mixer_out.shape, jnp.bfloat16),
            pltpu.VMEM((fs, blocks, depth, 2 * LANES), jnp.bfloat16),
            pltpu.VMEM((fs,) + down_proj.shape, jnp.bfloat16),
            pltpu.VMEM((tp, rows, own_width), jnp.bfloat16),
            pltpu.VMEM((tp, rows, channels), jnp.bfloat16),
            pltpu.VMEM((tp, rows, own_width), jnp.bfloat16),
            pltpu.VMEM((tp, rows, own_width), jnp.bfloat16),
            pltpu.VMEM((tp, blocks, rows, LANES), jnp.bfloat16),
            pltpu.VMEM((blocks, rows, LANES), jnp.bfloat16),
            pltpu.VMEM((rows, own_width), jnp.float32),
            pltpu.VMEM((rows, own_width), jnp.float32),
            pltpu.VMEM((2, tp, STAT_ROWS, rows), jnp.float32),
            pltpu.SemaphoreType.DMA((19,)),
            pltpu.SemaphoreType.DMA((sum(LANE_DEPTH.values()),)),
            pltpu.SemaphoreType.DMA((count, 3)),
            pltpu.SemaphoreType.DMA((count,)),
            pltpu.SemaphoreType.DMA((moves, 2)),
            pltpu.SemaphoreType.DMA((2,)),
            pltpu.SemaphoreType.DMA((GUEST_PARTS,)),
            pltpu.SemaphoreType.DMA((blocks * RETURN_PARTS,)),
        ],
        compiler_params=pltpu.CompilerParams(
            collective_id=0, has_side_effects=True, vmem_limit_bytes=60 * 1024 * 1024
        ),
    )(
        tokens,
        outer_gate,
        inner_gate,
        mixer_value,
        mixer_out,
        up_proj,
        gate_proj,
        down_proj,
        mixer_scales,
        mixer_taps,
        row(out_scale),
        row(first_gain),
        row(first_shift),
        up_scales,
        ffn_taps,
        ffn_shift,
        row(down_scale),
        row(second_gain),
        row(second_shift),
    )


def fits(mesh):
    return mesh.shape["rep"] == 2 and mesh.shape["fs"] == 4 and mesh.shape["tp"] == 4


def solution(mesh):
    body = functools.partial(fused, mesh.shape["fs"], mesh.shape["tp"]) if fits(mesh) else local
    return jax.shard_map(
        body,
        mesh=mesh,
        in_specs=(
            P(("rep", "fs"), "tp"),
            P("fs", "tp"),
            P("fs", "tp"),
            P("fs", "tp"),
            P(None, "tp"),
            P(None, "tp"),
            P("fs", "tp"),
            P("tp"),
            P(),
            P(),
            P("fs", "tp"),
            P("fs", "tp"),
            P(None, "tp"),
            P(None, None, "tp"),
            P(None, "tp"),
            P("fs", "tp"),
            P("tp"),
            P(),
            P(),
        ),
        out_specs=P(("rep", "fs"), "tp"),
        check_vma=False,
    )
```

```python
import functools

import jax
import jax.numpy as jnp
from jax import lax
from jax.experimental import pallas as pl
from jax.experimental.pallas import tpu as pltpu
from jax.sharding import PartitionSpec as P

LEN = 128


norm_eps = 1e-05
residual_weight = 8.0**0.25


def causal_mix(signal, kernel_taps):
    sequences = signal.reshape(-1, LEN, signal.shape[-1])
    padded = jnp.pad(sequences, ((0, 0), (2, 0), (0, 0)))
    mixed = (
        kernel_taps[0] * padded[:, :-2]
        + kernel_taps[1] * padded[:, 1:-1]
        + kernel_taps[2] * padded[:, 2:]
    )
    return mixed.reshape(signal.shape)


def lowered(matrix):
    return matrix.astype(jnp.bfloat16)


def single_fold(operand, portion):
    return jnp.dot(operand, portion, preferred_element_type=jnp.float32)


def fold_step(operand, pieces):
    result = []
    for number in range(len(pieces)):
        result.append(jnp.dot(operand, pieces[number], preferred_element_type=jnp.float32))
    return tuple(result)


def own_columns(vector, own_width):
    return lax.dynamic_slice_in_dim(vector, lax.axis_index("tp") * own_width, own_width, 0)


def scaled_norm(summed, average, spread, gain_vector, shift_vector):
    return (summed - average) * lax.rsqrt(spread + norm_eps) * gain_vector + shift_vector


def local(
    tokens,
    outer_gate,
    inner_gate,
    mixer_value,
    mixer_scales,
    mixer_taps,
    mixer_out,
    out_scale,
    first_gain,
    first_shift,
    up_proj,
    gate_proj,
    up_scales,
    ffn_taps,
    ffn_shift,
    down_proj,
    down_scale,
    second_gain,
    second_shift,
):
    own_width = tokens.shape[1]
    full_width = own_width * lax.axis_size("tp")
    token_whole = lax.all_gather(tokens, "tp", axis=1, tiled=True)
    outer_part, inner_part, value_part = fold_step(
        token_whole,
        (
            lax.all_gather(lowered(outer_gate), "fs", axis=0, tiled=True),
            lax.all_gather(lowered(inner_gate), "fs", axis=0, tiled=True),
            lax.all_gather(lowered(mixer_value), "fs", axis=0, tiled=True),
        ),
    )
    outer_part = (outer_part * mixer_scales[0]).astype(jnp.bfloat16)
    inner_part = (inner_part * mixer_scales[1]).astype(jnp.bfloat16)
    value_part = (value_part * mixer_scales[2]).astype(jnp.bfloat16)
    product = inner_part.astype(jnp.float32) * value_part.astype(jnp.float32)
    mixed_conv = (outer_part.astype(jnp.float32) * causal_mix(product, mixer_taps)).astype(
        jnp.bfloat16
    )
    conv_whole = lax.all_gather(mixed_conv, "tp", axis=1, tiled=True)
    mixer_sum = (
        single_fold(conv_whole, lax.all_gather(lowered(mixer_out), "fs", axis=0, tiled=True))
        * out_scale
    )
    first_sum = residual_weight * tokens.astype(jnp.float32) + mixer_sum
    row_total, row_square = lax.psum(
        (jnp.sum(first_sum, 1, keepdims=True), jnp.sum(first_sum * first_sum, 1, keepdims=True)),
        "tp",
    )
    average = row_total / full_width
    spread = row_square / full_width - average * average
    normed = scaled_norm(
        first_sum,
        average,
        spread,
        own_columns(first_gain, own_width),
        own_columns(first_shift, own_width),
    ).astype(jnp.bfloat16)
    normed_whole = lax.all_gather(normed, "tp", axis=1, tiled=True)
    up_matrix, gate_matrix = (
        lax.all_gather(lowered(up_proj), "fs", axis=0, tiled=True),
        lax.all_gather(lowered(gate_proj), "fs", axis=0, tiled=True),
    )
    up_linear = jnp.dot(normed_whole, up_matrix, preferred_element_type=jnp.float32)
    gate_linear = jnp.dot(normed_whole, gate_matrix, preferred_element_type=jnp.float32)
    up_linear = up_linear * up_scales[0]
    gate_linear = gate_linear * up_scales[1]
    up_mixed = causal_mix(up_linear, ffn_taps[:, 0]) + ffn_shift[0]
    gate_mixed = causal_mix(gate_linear, ffn_taps[:, 1]) + ffn_shift[1]
    hidden = (up_mixed * jax.nn.silu(gate_mixed)).astype(jnp.bfloat16)
    hidden_whole = lax.all_gather(hidden, "tp", axis=1, tiled=True)
    ffn_sum = (
        single_fold(hidden_whole, lax.all_gather(lowered(down_proj), "fs", axis=0, tiled=True))
        * down_scale
    )
    second_sum = residual_weight * normed.astype(jnp.float32) + ffn_sum
    second_total, second_square = lax.psum(
        (jnp.sum(second_sum, 1, keepdims=True), jnp.sum(second_sum * second_sum, 1, keepdims=True)),
        "tp",
    )
    second_average = second_total / full_width
    second_spread = second_square / full_width - second_average * second_average
    return scaled_norm(
        second_sum,
        second_average,
        second_spread,
        own_columns(second_gain, own_width),
        own_columns(second_shift, own_width),
    ).astype(jnp.bfloat16)


LANES = 128
STAT_ROWS = 2
GUEST_PARTS = 4
CONV_PARTS = 2
ROW_CUT = 128
RETURN_PARTS = 2
MIX_PARTS = 4
BLOCK_PARTS = (1, 1, 1, 1, 1, 2)
LANE_DEPTH = {"zi": 14, "zo": 8, "y": 8, "x": 8, "d": 8}


def shifted_mix(signal, first, second, third):
    rows = lax.broadcasted_iota(jnp.int32, signal.shape, 0) % LEN
    one = jnp.where(rows >= 1, pltpu.roll(signal, 1, 0), 0.0)
    two = jnp.where(rows >= 2, pltpu.roll(signal, 2, 0), 0.0)
    return first * two + second * one + third * signal


def dot32(left, right):
    return jnp.dot(left, right, preferred_element_type=jnp.float32)


def kernel(
    fs,
    tp,
    tokens_hbm,
    outer_hbm,
    inner_hbm,
    value_hbm,
    out_hbm,
    up_hbm,
    gate_hbm,
    down_hbm,
    mixer_scales_hbm,
    mixer_taps_hbm,
    out_scale_hbm,
    first_gain_hbm,
    first_shift_hbm,
    up_scales_hbm,
    ffn_taps_hbm,
    ffn_shift_hbm,
    down_scale_hbm,
    second_gain_hbm,
    second_shift_hbm,
    result,
    mix_f,
    out_f,
    up_f,
    gate_f,
    down_f,
    mixer_scales,
    mixer_taps,
    out_scale,
    first_gain,
    first_shift,
    up_scales,
    ffn_taps,
    ffn_shift,
    down_scale,
    second_gain,
    second_shift,
    mix_g,
    out_g,
    ug_g,
    down_g,
    token_all,
    conv_all,
    norm_all,
    guest_all,
    hidden_all,
    hidden_out,
    first_sum,
    total,
    stats,
    load_sem,
    send_sem,
    arrive_sem,
    gather_sem,
    recv_x,
    recv_s,
    recv_g,
):
    r, z, t = lax.axis_index("rep"), lax.axis_index("fs"), lax.axis_index("tp")
    sibling = t + 1 - 2 * (t % 2)
    across = (t + 2) % tp
    diagonal = (sibling + 2) % tp
    other = 1 - r
    rows, own_width = result.shape
    full_width = own_width * tp
    channels = conv_all.shape[2]
    blocks = ug_g.shape[1]
    last = fs - 1
    own_lanes = pl.ds(pl.multiple_of(t * own_width, own_width), own_width)

    sources = (tokens_hbm, outer_hbm, inner_hbm, value_hbm, out_hbm, up_hbm, gate_hbm, down_hbm)
    sources += (mixer_scales_hbm, mixer_taps_hbm, out_scale_hbm, first_gain_hbm.at[:, own_lanes])
    sources += (first_shift_hbm.at[:, own_lanes], up_scales_hbm, ffn_taps_hbm, ffn_shift_hbm, down_scale_hbm)
    sources += (second_gain_hbm.at[:, own_lanes], second_shift_hbm.at[:, own_lanes])
    places = (token_all.at[t], mix_f.at[0], mix_f.at[1], mix_f.at[2], out_f, up_f, gate_f, down_f)
    places += (mixer_scales, mixer_taps, out_scale, first_gain, first_shift, up_scales, ffn_taps, ffn_shift)
    places += (down_scale, second_gain, second_shift)
    loads = [
        pltpu.make_async_copy(source, place, load_sem.at[max(number - 2, min(number, 1))])
        for number, (source, place) in enumerate(zip(sources, places))
    ]
    for load in loads:
        load.start()

    barrier = pltpu.get_barrier_semaphore()
    for peer in (sibling, across, diagonal):
        pl.semaphore_signal(barrier, inc=1, device_id={"tp": peer}, device_id_type=pl.DeviceIdType.MESH)
    pl.semaphore_signal(barrier, inc=1, device_id={"rep": other}, device_id_type=pl.DeviceIdType.MESH)

    @pl.when(z > 0)
    def _():
        pl.semaphore_signal(barrier, inc=1, device_id={"fs": z - 1}, device_id_type=pl.DeviceIdType.MESH)

    @pl.when(z < last)
    def _():
        pl.semaphore_signal(barrier, inc=1, device_id={"fs": z + 1}, device_id_type=pl.DeviceIdType.MESH)

    inside = (z > 0) & (z < last)

    @pl.when(inside)
    def _():
        pl.semaphore_wait(barrier, 6)

    @pl.when(jnp.logical_not(inside))
    def _():
        pl.semaphore_wait(barrier, 5)

    guest_rows = rows // GUEST_PARTS
    return_rows = rows // RETURN_PARTS
    norm_move = 1 + CONV_PARTS
    first_hidden, first_guest = norm_move + 1, norm_move + 1 + blocks * RETURN_PARTS
    conv_rows = rows // CONV_PARTS

    def offset(value, size):
        return value if isinstance(value, int) else pl.multiple_of(value, size)

    def mix_unit(part):
        size = mix_g.shape[1] // (2 * MIX_PARTS)
        return lambda source, half: mix_g.at[source, pl.ds(offset((part * 2 + half) * size, size), size)]

    def out_unit(source, half):
        size = out_g.shape[1] // 2
        return out_g.at[source, pl.ds(offset(half * size, size), size)]

    def ug_unit(block, part):
        size = ug_g.shape[2] // (2 * BLOCK_PARTS[block])
        return lambda source, half: ug_g.at[
            source, block, pl.ds(offset((part * 2 + half) * size, size), size)
        ]

    def down_unit(part):
        size = LANES
        return lambda source, half: down_g.at[source, pl.ds(offset((part * 2 + half) * size, size), size)]

    parts = blocks // 2
    units = [mix_unit(part) for part in range(MIX_PARTS)] + [out_unit]
    out_index, first_down = MIX_PARTS, MIX_PARTS + 1
    units += [down_unit(part) for part in range(parts)]
    first_ug = len(units)
    block_units = []
    for block in range(blocks):
        block_units.append(range(len(units), len(units) + BLOCK_PARTS[block]))
        units += [ug_unit(block, part) for part in range(BLOCK_PARTS[block])]
    count = len(units)

    def program(middle):
        if middle:
            outer, inner, far = (z - 1) * last, last - z, (2 - z) * last
        else:
            near = 1 + z // last
            beyond, far = last - near, last - z
        queues, lowered_blocks = {name: [] for name in LANE_DEPTH}, []
        bases = {}
        for name, depth in LANE_DEPTH.items():
            bases[name] = sum(LANE_DEPTH[other_name] for other_name in bases)

        def send(lane, source, target, recv_sem, device):
            queue, depth = queues[lane], LANE_DEPTH[lane]
            if len(queue) >= depth:
                queue[-depth].wait_send()
            copy = pltpu.make_async_remote_copy(
                src_ref=source,
                dst_ref=target,
                send_sem=send_sem.at[bases[lane] + len(queue) % depth],
                recv_sem=recv_sem,
                device_id=device,
                device_id_type=pl.DeviceIdType.MESH,
            )
            copy.start()
            queue.append(copy)

        def arrived(ref, recv_sem):
            pltpu.make_async_remote_copy(
                src_ref=ref,
                dst_ref=ref,
                send_sem=send_sem.at[0],
                recv_sem=recv_sem,
                device_id={"tp": sibling},
                device_id_type=pl.DeviceIdType.MESH,
            ).wait_recv()

        def moved(number, slot):
            if number == 0:
                return token_all.at[slot]
            if number < norm_move:
                return conv_all.at[slot, pl.ds((number - 1) * conv_rows, conv_rows)]
            if number == norm_move:
                return norm_all.at[slot]
            if number >= first_guest:
                return guest_all.at[slot, pl.ds((number - first_guest) * guest_rows, guest_rows)]
            block, part = (number - first_hidden) // RETURN_PARTS, (number - first_hidden) % RETURN_PARTS
            if middle:
                return hidden_all.at[slot, block]
            return hidden_all.at[slot, block, pl.ds(part * return_rows, return_rows)]

        def exchange_start(number):
            if number == 0:
                loads[0].wait()
            send("x", moved(number, t), moved(number, t), recv_x.at[number, 0], {"tp": across})
            send("d", moved(number, t), moved(number, t), recv_x.at[number, 1], {"tp": sibling})

        def exchange_pass(number):
            arrived(moved(number, across), recv_x.at[number, 0])
            send("d", moved(number, across), moved(number, across), recv_x.at[number, 1], {"tp": sibling})

        def exchange_end(number):
            arrived(moved(number, pl.ds(0, 2)), recv_x.at[number, 1])

        def own(unit):
            ref = units[unit](z, r)
            if middle:
                send("zi", ref, ref, arrive_sem.at[unit, 1], {"fs": inner})
                if unit < first_ug:
                    send("zo", ref, ref, arrive_sem.at[unit, 0], {"fs": outer})
            else:
                send("zi", ref, ref, arrive_sem.at[unit, 0], {"fs": near})

        def own_rest(unit):
            ref = units[unit](z, other)
            send("zi", ref, ref, gather_sem.at[unit], {"fs": near})

        def from_outer(unit):
            ref = units[unit](outer, r)
            arrived(ref, arrive_sem.at[unit, 0])
            send("zi", ref, ref, arrive_sem.at[unit, 2], {"fs": inner})

        def from_inner(unit, source, place):
            ref = units[unit](source, r)
            arrived(ref, arrive_sem.at[unit, place])
            send("y", ref, ref, gather_sem.at[unit], {"rep": other})
            if middle and unit < first_ug:
                send("zo", ref, ref, arrive_sem.at[unit, place], {"fs": outer})

        def need(unit):
            arrived(units[unit](pl.ds(0, 3), 0), gather_sem.at[unit])

        def lower_mix():
            pltpu.make_async_copy(mix_f, mix_f, load_sem.at[1]).wait()
            for part in range(3):
                mix_g[z, :, part * channels : (part + 1) * channels] = mix_f[part].astype(jnp.bfloat16)

        def lower_out():
            loads[4].wait()
            out_g[z] = out_f[...].astype(jnp.bfloat16)

        def lower_down():
            loads[7].wait()
            down_g[z] = down_f[...].astype(jnp.bfloat16)

        def small_loads():
            for load in loads[8:]:
                load.wait()

        def lower_block(block):
            if not lowered_blocks:
                loads[5].wait()
                loads[6].wait()
            lowered_blocks.append(block)
            columns = slice(block * LANES, (block + 1) * LANES)
            ug_g[z, block, :, :LANES] = up_f[:, columns].astype(jnp.bfloat16)
            ug_g[z, block, :, LANES:] = gate_f[:, columns].astype(jnp.bfloat16)

        def sums_start(number, summed):
            lane = lax.broadcasted_iota(jnp.int32, (rows, LANES), 1)
            one = jnp.sum(summed, axis=1, keepdims=True)
            two = jnp.sum(summed * summed, axis=1, keepdims=True)
            stats[number, t] = jnp.transpose(jnp.where(lane == 0, one, two))[:STAT_ROWS]
            ref = stats.at[number, t]
            for lane_name, peer in (("x", across), ("x", diagonal), ("d", sibling)):
                send(lane_name, ref, ref, recv_s.at[number], {"tp": peer})

        def sums_end(number):
            arrived(stats.at[number, pl.ds(0, 3)], recv_s.at[number])
            summed = stats[number, 0]
            for slot in range(1, tp):
                summed = summed + stats[number, slot]
            back = jnp.transpose(jnp.concatenate([summed] * (LANES // STAT_ROWS), axis=0))
            average = back[:, 0:1] / full_width
            return average, back[:, 1:2] / full_width - average * average

        def mixer(part):
            if part == 0:
                for unit in range(MIX_PARTS):
                    need(unit)
                exchange_end(0)
            lines = slice(part * conv_rows, (part + 1) * conv_rows)
            gathered = dot32(token_all[0, lines], mix_g[0])
            for slot in range(1, tp):
                gathered = gathered + dot32(token_all[slot, lines], mix_g[slot])
            scaled = [
                (gathered[:, kind * channels : (kind + 1) * channels] * mixer_scales[kind : kind + 1])
                .astype(jnp.bfloat16)
                .astype(jnp.float32)
                for kind in range(3)
            ]
            mixed = scaled[0] * shifted_mix(
                scaled[1] * scaled[2], mixer_taps[0:1], mixer_taps[1:2], mixer_taps[2:3]
            )
            conv_all[t, lines] = mixed.astype(jnp.bfloat16)
            exchange_start(1 + part)

        def mixer_output():
            need(out_index)
            for part in range(CONV_PARTS):
                exchange_end(1 + part)
            summed = dot32(conv_all[0], out_g[0])
            for slot in range(1, tp):
                summed = summed + dot32(conv_all[slot], out_g[slot])
            summed = summed * out_scale[...] + residual_weight * token_all[t].astype(jnp.float32)
            first_sum[...] = summed
            sums_start(0, summed)

        def first_norm():
            average, spread = sums_end(0)
            norm_all[t] = scaled_norm(
                first_sum[...], average, spread, first_gain[...], first_shift[...]
            ).astype(jnp.bfloat16)

        def guest_send(part):
            lines = pl.ds(part * guest_rows, guest_rows)
            send("zi", norm_all.at[t, lines], guest_all.at[t, lines], recv_g.at[part], {"fs": near})

        def units_of(block, left, lines):
            both = dot32(left(0, lines), ug_g[0, block])
            for slot in range(1, tp):
                both = both + dot32(left(slot, lines), ug_g[slot, block])
            columns = slice(block * LANES, (block + 1) * LANES)
            mixed = []
            for side in range(2):
                mixed.append(
                    shifted_mix(
                        both[:, side * LANES : (side + 1) * LANES] * up_scales[side : side + 1, columns],
                        ffn_taps[0, side : side + 1, columns],
                        ffn_taps[1, side : side + 1, columns],
                        ffn_taps[2, side : side + 1, columns],
                    )
                    + ffn_shift[side : side + 1, columns]
                )
            return (mixed[0] * mixed[1] / (1.0 + jnp.exp(-mixed[1]))).astype(jnp.bfloat16)

        row_cuts = [slice(first, first + ROW_CUT) for first in range(0, rows, ROW_CUT)]

        def store_units(block, left, target):
            for lines in row_cuts:
                target[lines] = units_of(block, lambda slot, lines: left[slot, lines], lines)

        def back_sem(number):
            return arrive_sem.at[first_ug + number // 3, number % 3]

        def need_block(block):
            for unit in block_units[block]:
                need(unit)

        def hidden(block):
            store_units(block, norm_all, hidden_all.at[t, block])
            exchange_start(first_hidden + block * RETURN_PARTS)

        def give_back(block):
            for part in range(RETURN_PARTS):
                lines = pl.ds(part * return_rows, return_rows)
                number = block * RETURN_PARTS + part
                send(
                    "zo", hidden_out.at[block, lines], hidden_all.at[t, block, lines], back_sem(number), {"fs": outer}
                )

        def guest_hidden(block):
            store_units(block, guest_all, hidden_out.at[block])
            give_back(block)

        def both_hidden(block):
            store_units(block, guest_all, hidden_out.at[block])
            store_units(block, norm_all, hidden_all.at[t, block])
            give_back(block)
            exchange_start(first_hidden + block * RETURN_PARTS)

        def guest_start(part):
            lines = pl.ds(part * guest_rows, guest_rows)
            arrived(guest_all.at[t, lines], recv_g.at[part])
            exchange_start(first_guest + part)

        def returned(number):
            arrived(moved(first_hidden + number, t), back_sem(number))
            exchange_start(first_hidden + number)

        def hidden_end(block):
            for part in range(1 if middle else RETURN_PARTS):
                exchange_end(first_hidden + block * RETURN_PARTS + part)

        def down(part):
            need(first_down + part)
            for block in (2 * part, 2 * part + 1):
                hidden_end(block)
            summed = None
            for slot in range(tp):
                left = jnp.concatenate([hidden_all[slot, 2 * part], hidden_all[slot, 2 * part + 1]], axis=1)
                term = dot32(left, down_g[slot, part * 2 * LANES : (part + 1) * 2 * LANES])
                summed = term if summed is None else summed + term
            total[...] = summed if part == 0 else total[...] + summed

        def finish():
            second = total[...] * down_scale[...] + residual_weight * norm_all[t].astype(jnp.float32)
            total[...] = second
            sums_start(1, second)
            average, spread = sums_end(1)
            result[...] = scaled_norm(total[...], average, spread, second_gain[...], second_shift[...]).astype(
                result.dtype
            )
            for name, queue in queues.items():
                for copy in queue[-LANE_DEPTH[name] :]:
                    copy.wait_send()

        if middle:
            lower_mix()
            own(1)
            own(2)
            lower_out()
            exchange_start(0)
            lower_down()
            own(0)
            lower_block(2)
            own(3)
            lower_block(1)
            from_outer(0)
            from_inner(1, inner, 1)
            from_outer(3)
            from_inner(2, inner, 1)
            from_inner(0, inner, 1)
            from_outer(1)
            own(4)
            from_outer(2)
            from_inner(3, far, 2)
            lower_block(4)
            from_outer(4)
            own(9)
            from_inner(1, far, 2)
            from_inner(0, far, 2)
            from_inner(3, inner, 1)
            own(12)
            from_inner(2, far, 2)
            lower_block(3)
            from_inner(4, far, 2)
            small_loads()
            from_inner(4, inner, 1)
            lower_block(0)
            own(5)
            exchange_pass(0)
            from_outer(7)
            from_inner(9, inner, 1)
            mixer(0)
            mixer(1)
            own(6)
            from_outer(9)
            from_inner(12, inner, 1)
            exchange_pass(1)
            own(7)
            exchange_pass(2)
            from_inner(5, inner, 1)
            mixer_output()
            from_inner(7, far, 2)
            from_inner(6, inner, 1)
            from_outer(8)
            first_norm()
            exchange_start(3)
            from_inner(9, far, 2)
            from_outer(5)
            lower_block(5)
            own(8)
            from_outer(10)
            from_inner(7, inner, 1)
            from_inner(8, far, 2)
            from_inner(5, far, 2)
            guest_start(2)
            from_inner(8, inner, 1)
            from_outer(6)
            own(10)
            from_outer(11)
            guest_start(0)
            exchange_pass(3)
            guest_start(1)
            from_inner(10, far, 2)
            from_inner(6, far, 2)
            own(11)
            guest_start(3)
            exchange_pass(16)
            from_inner(10, inner, 1)
            exchange_pass(18)
            exchange_pass(17)
            from_outer(12)
            from_outer(14)
            from_inner(11, far, 2)
            exchange_pass(19)
            from_outer(13)
            exchange_end(3)
            need_block(0)
            from_inner(11, inner, 1)
            exchange_end(18)
            need_block(1)
            exchange_end(16)
            exchange_end(19)
            exchange_end(17)
            guest_hidden(0)
            hidden(1)
            own(14)
            need_block(2)
            from_inner(12, far, 2)
            guest_hidden(1)
            own(13)
            hidden(0)
            from_inner(14, far, 2)
            guest_hidden(2)
            from_inner(13, far, 2)
            need_block(3)
            hidden(2)
            from_inner(14, inner, 1)
            from_inner(13, inner, 1)
            guest_hidden(3)
            need_block(4)
            hidden(4)
            guest_hidden(4)
            exchange_pass(6)
            hidden(3)
            need_block(5)
            exchange_pass(4)
            guest_hidden(5)
            exchange_pass(8)
            hidden(5)
            down(0)
            exchange_pass(10)
            exchange_pass(12)
            exchange_pass(14)
            down(1)
            down(2)
            finish()
        else:
            lower_mix()
            own(0)
            own(3)
            small_loads()
            own(1)
            lower_out()
            lower_down()
            own(2)
            own(4)
            own(7)
            exchange_start(0)
            lower_block(0)
            own_rest(2)
            from_inner(2, near, 0)
            from_inner(0, near, 0)
            lower_block(1)
            from_inner(1, near, 0)
            lower_block(4)
            own_rest(3)
            lower_block(5)
            from_inner(1, beyond, 1)
            own_rest(1)
            own_rest(4)
            own_rest(0)
            from_inner(3, near, 0)
            own(9)
            own(6)
            from_inner(2, beyond, 1)
            own(8)
            from_inner(0, beyond, 1)
            own(12)
            from_inner(3, far, 2)
            from_inner(1, far, 2)
            from_inner(0, far, 2)
            exchange_pass(0)
            from_inner(3, beyond, 1)
            own(5)
            lower_block(3)
            from_inner(2, far, 2)
            from_inner(4, far, 2)
            mixer(0)
            mixer(1)
            lower_block(2)
            own(10)
            from_inner(4, beyond, 1)
            from_inner(4, near, 0)
            exchange_pass(1)
            own(11)
            exchange_pass(2)
            mixer_output()
            first_norm()
            guest_send(2)
            guest_send(0)
            guest_send(1)
            own(14)
            guest_send(3)
            own(13)
            own_rest(8)
            own_rest(9)
            own_rest(10)
            own_rest(11)
            from_inner(5, near, 0)
            from_inner(5, beyond, 1)
            from_inner(7, beyond, 1)
            own_rest(12)
            own_rest(13)
            returned(0)
            from_inner(6, near, 0)
            own_rest(14)
            from_inner(6, beyond, 1)
            own_rest(6)
            returned(1)
            returned(2)
            returned(3)
            returned(4)
            from_inner(7, near, 0)
            returned(5)
            exchange_pass(4)
            from_inner(5, far, 2)
            own_rest(5)
            returned(6)
            own_rest(7)
            from_inner(7, far, 2)
            returned(7)
            exchange_pass(7)
            exchange_pass(5)
            from_inner(6, far, 2)
            returned(8)
            returned(9)
            exchange_pass(6)
            returned(10)
            returned(11)
            exchange_pass(9)
            exchange_pass(14)
            exchange_pass(13)
            exchange_pass(8)
            exchange_pass(11)
            exchange_pass(10)
            exchange_pass(12)
            down(0)
            exchange_pass(15)
            down(1)
            down(2)
            finish()
    @pl.when(inside)
    def _():
        program(True)

    @pl.when(jnp.logical_not(inside))
    def _():
        program(False)


def fused(
    fs,
    tp,
    tokens,
    outer_gate,
    inner_gate,
    mixer_value,
    mixer_scales,
    mixer_taps,
    mixer_out,
    out_scale,
    first_gain,
    first_shift,
    up_proj,
    gate_proj,
    up_scales,
    ffn_taps,
    ffn_shift,
    down_proj,
    down_scale,
    second_gain,
    second_shift,
):
    rows, own_width = tokens.shape
    depth, channels = outer_gate.shape
    hidden = up_proj.shape[1]
    blocks = hidden // LANES
    count = MIX_PARTS + 1 + blocks // 2 + sum(BLOCK_PARTS)
    moves = 2 + CONV_PARTS + blocks * RETURN_PARTS + GUEST_PARTS
    any_space = pl.BlockSpec(memory_space=pl.ANY)
    in_vmem = pl.BlockSpec(memory_space=pltpu.VMEM)

    def row(vector):
        return vector.reshape(1, -1)

    return pl.pallas_call(
        functools.partial(kernel, fs, tp),
        out_shape=jax.ShapeDtypeStruct((rows, own_width), jnp.bfloat16),
        in_specs=[any_space] * 19,
        out_specs=in_vmem,
        scratch_shapes=[
            pltpu.VMEM((3, depth, channels), jnp.float32),
            pltpu.VMEM(mixer_out.shape, jnp.float32),
            pltpu.VMEM(up_proj.shape, jnp.float32),
            pltpu.VMEM(gate_proj.shape, jnp.float32),
            pltpu.VMEM(down_proj.shape, jnp.float32),
            pltpu.VMEM(mixer_scales.shape, jnp.float32),
            pltpu.VMEM(mixer_taps.shape, jnp.float32),
            pltpu.VMEM((1, own_width), jnp.float32),
            pltpu.VMEM((1, own_width), jnp.float32),
            pltpu.VMEM((1, own_width), jnp.float32),
            pltpu.VMEM(up_scales.shape, jnp.float32),
            pltpu.VMEM(ffn_taps.shape, jnp.float32),
            pltpu.VMEM(ffn_shift.shape, jnp.float32),
            pltpu.VMEM((1, own_width), jnp.float32),
            pltpu.VMEM((1, own_width), jnp.float32),
            pltpu.VMEM((1, own_width), jnp.float32),
            pltpu.VMEM((fs, depth, 3 * channels), jnp.bfloat16),
            pltpu.VMEM((fs,) + mixer_out.shape, jnp.bfloat16),
            pltpu.VMEM((fs, blocks, depth, 2 * LANES), jnp.bfloat16),
            pltpu.VMEM((fs,) + down_proj.shape, jnp.bfloat16),
            pltpu.VMEM((tp, rows, own_width), jnp.bfloat16),
            pltpu.VMEM((tp, rows, channels), jnp.bfloat16),
            pltpu.VMEM((tp, rows, own_width), jnp.bfloat16),
            pltpu.VMEM((tp, rows, own_width), jnp.bfloat16),
            pltpu.VMEM((tp, blocks, rows, LANES), jnp.bfloat16),
            pltpu.VMEM((blocks, rows, LANES), jnp.bfloat16),
            pltpu.VMEM((rows, own_width), jnp.float32),
            pltpu.VMEM((rows, own_width), jnp.float32),
            pltpu.VMEM((2, tp, STAT_ROWS, rows), jnp.float32),
            pltpu.SemaphoreType.DMA((17,)),
            pltpu.SemaphoreType.DMA((sum(LANE_DEPTH.values()),)),
            pltpu.SemaphoreType.DMA((count, 3)),
            pltpu.SemaphoreType.DMA((count,)),
            pltpu.SemaphoreType.DMA((moves, 2)),
            pltpu.SemaphoreType.DMA((2,)),
            pltpu.SemaphoreType.DMA((GUEST_PARTS,)),
        ],
        compiler_params=pltpu.CompilerParams(
            collective_id=0, has_side_effects=True, vmem_limit_bytes=60 * 1024 * 1024
        ),
    )(
        tokens,
        outer_gate,
        inner_gate,
        mixer_value,
        mixer_out,
        up_proj,
        gate_proj,
        down_proj,
        mixer_scales,
        mixer_taps,
        row(out_scale),
        row(first_gain),
        row(first_shift),
        up_scales,
        ffn_taps,
        ffn_shift,
        row(down_scale),
        row(second_gain),
        row(second_shift),
    )


def fits(mesh):
    return mesh.shape["rep"] == 2 and mesh.shape["fs"] == 4 and mesh.shape["tp"] == 4


def solution(mesh):
    body = functools.partial(fused, mesh.shape["fs"], mesh.shape["tp"]) if fits(mesh) else local
    return jax.shard_map(
        body,
        mesh=mesh,
        in_specs=(
            P(("rep", "fs"), "tp"),
            P("fs", "tp"),
            P("fs", "tp"),
            P("fs", "tp"),
            P(None, "tp"),
            P(None, "tp"),
            P("fs", "tp"),
            P("tp"),
            P(),
            P(),
            P("fs", "tp"),
            P("fs", "tp"),
            P(None, "tp"),
            P(None, None, "tp"),
            P(None, "tp"),
            P("fs", "tp"),
            P("tp"),
            P(),
            P(),
        ),
        out_specs=P(("rep", "fs"), "tp"),
        check_vma=False,
    )
```

```python
import functools

import jax
import jax.numpy as jnp
from jax import lax
from jax.experimental import pallas as pl
from jax.experimental.pallas import tpu as pltpu
from jax.sharding import PartitionSpec as P

LEN = 128


norm_eps = 1e-05
residual_weight = 8.0**0.25


def causal_mix(signal, kernel_taps):
    sequences = signal.reshape(-1, LEN, signal.shape[-1])
    padded = jnp.pad(sequences, ((0, 0), (2, 0), (0, 0)))
    mixed = (
        kernel_taps[0] * padded[:, :-2]
        + kernel_taps[1] * padded[:, 1:-1]
        + kernel_taps[2] * padded[:, 2:]
    )
    return mixed.reshape(signal.shape)


def lowered(matrix):
    return matrix.astype(jnp.bfloat16)


def single_fold(operand, portion):
    return jnp.dot(operand, portion, preferred_element_type=jnp.float32)


def fold_step(operand, pieces):
    result = []
    for number in range(len(pieces)):
        result.append(jnp.dot(operand, pieces[number], preferred_element_type=jnp.float32))
    return tuple(result)


def own_columns(vector, own_width):
    return lax.dynamic_slice_in_dim(vector, lax.axis_index("tp") * own_width, own_width, 0)


def scaled_norm(summed, average, spread, gain_vector, shift_vector):
    return (summed - average) * lax.rsqrt(spread + norm_eps) * gain_vector + shift_vector


def local(
    tokens,
    outer_gate,
    inner_gate,
    mixer_value,
    mixer_scales,
    mixer_taps,
    mixer_out,
    out_scale,
    first_gain,
    first_shift,
    up_proj,
    gate_proj,
    up_scales,
    ffn_taps,
    ffn_shift,
    down_proj,
    down_scale,
    second_gain,
    second_shift,
):
    own_width = tokens.shape[1]
    full_width = own_width * lax.axis_size("tp")
    token_whole = lax.all_gather(tokens, "tp", axis=1, tiled=True)
    outer_part, inner_part, value_part = fold_step(
        token_whole,
        (
            lax.all_gather(lowered(outer_gate), "fs", axis=0, tiled=True),
            lax.all_gather(lowered(inner_gate), "fs", axis=0, tiled=True),
            lax.all_gather(lowered(mixer_value), "fs", axis=0, tiled=True),
        ),
    )
    outer_part = (outer_part * mixer_scales[0]).astype(jnp.bfloat16)
    inner_part = (inner_part * mixer_scales[1]).astype(jnp.bfloat16)
    value_part = (value_part * mixer_scales[2]).astype(jnp.bfloat16)
    product = inner_part.astype(jnp.float32) * value_part.astype(jnp.float32)
    mixed_conv = (outer_part.astype(jnp.float32) * causal_mix(product, mixer_taps)).astype(
        jnp.bfloat16
    )
    conv_whole = lax.all_gather(mixed_conv, "tp", axis=1, tiled=True)
    mixer_sum = (
        single_fold(conv_whole, lax.all_gather(lowered(mixer_out), "fs", axis=0, tiled=True))
        * out_scale
    )
    first_sum = residual_weight * tokens.astype(jnp.float32) + mixer_sum
    row_total, row_square = lax.psum(
        (jnp.sum(first_sum, 1, keepdims=True), jnp.sum(first_sum * first_sum, 1, keepdims=True)),
        "tp",
    )
    average = row_total / full_width
    spread = row_square / full_width - average * average
    normed = scaled_norm(
        first_sum,
        average,
        spread,
        own_columns(first_gain, own_width),
        own_columns(first_shift, own_width),
    ).astype(jnp.bfloat16)
    normed_whole = lax.all_gather(normed, "tp", axis=1, tiled=True)
    up_matrix, gate_matrix = (
        lax.all_gather(lowered(up_proj), "fs", axis=0, tiled=True),
        lax.all_gather(lowered(gate_proj), "fs", axis=0, tiled=True),
    )
    up_linear = jnp.dot(normed_whole, up_matrix, preferred_element_type=jnp.float32)
    gate_linear = jnp.dot(normed_whole, gate_matrix, preferred_element_type=jnp.float32)
    up_linear = up_linear * up_scales[0]
    gate_linear = gate_linear * up_scales[1]
    up_mixed = causal_mix(up_linear, ffn_taps[:, 0]) + ffn_shift[0]
    gate_mixed = causal_mix(gate_linear, ffn_taps[:, 1]) + ffn_shift[1]
    hidden = (up_mixed * jax.nn.silu(gate_mixed)).astype(jnp.bfloat16)
    hidden_whole = lax.all_gather(hidden, "tp", axis=1, tiled=True)
    ffn_sum = (
        single_fold(hidden_whole, lax.all_gather(lowered(down_proj), "fs", axis=0, tiled=True))
        * down_scale
    )
    second_sum = residual_weight * normed.astype(jnp.float32) + ffn_sum
    second_total, second_square = lax.psum(
        (jnp.sum(second_sum, 1, keepdims=True), jnp.sum(second_sum * second_sum, 1, keepdims=True)),
        "tp",
    )
    second_average = second_total / full_width
    second_spread = second_square / full_width - second_average * second_average
    return scaled_norm(
        second_sum,
        second_average,
        second_spread,
        own_columns(second_gain, own_width),
        own_columns(second_shift, own_width),
    ).astype(jnp.bfloat16)


LANES = 128
STAT_ROWS = 2
GUEST_PARTS = 4
CONV_PARTS = 2
ROW_CUT = 256
RETURN_PARTS = 2
MIX_PARTS = 4
BLOCK_PARTS = (1, 1, 1, 1, 1, 2)
LANE_DEPTH = {"zi": 14, "zo": 6, "y": 6, "x": 6, "d": 6}


def shifted_mix(signal, first, second, third):
    rows = lax.broadcasted_iota(jnp.int32, signal.shape, 0) % LEN
    one = jnp.where(rows >= 1, pltpu.roll(signal, 1, 0), 0.0)
    two = jnp.where(rows >= 2, pltpu.roll(signal, 2, 0), 0.0)
    return first * two + second * one + third * signal


def dot32(left, right):
    return jnp.dot(left, right, preferred_element_type=jnp.float32)


def kernel(
    fs,
    tp,
    tokens_hbm,
    outer_hbm,
    inner_hbm,
    value_hbm,
    out_hbm,
    up_hbm,
    gate_hbm,
    down_hbm,
    mixer_scales_hbm,
    mixer_taps_hbm,
    out_scale_hbm,
    first_gain_hbm,
    first_shift_hbm,
    up_scales_hbm,
    ffn_taps_hbm,
    ffn_shift_hbm,
    down_scale_hbm,
    second_gain_hbm,
    second_shift_hbm,
    result,
    mix_f,
    out_f,
    up_f,
    gate_f,
    down_f,
    mixer_scales,
    mixer_taps,
    out_scale,
    first_gain,
    first_shift,
    up_scales,
    ffn_taps,
    ffn_shift,
    down_scale,
    second_gain,
    second_shift,
    mix_g,
    out_g,
    ug_g,
    down_g,
    token_all,
    conv_all,
    norm_all,
    guest_all,
    hidden_all,
    hidden_out,
    first_sum,
    total,
    stats,
    load_sem,
    send_sem,
    arrive_sem,
    gather_sem,
    recv_x,
    recv_s,
    recv_g,
):
    r, z, t = lax.axis_index("rep"), lax.axis_index("fs"), lax.axis_index("tp")
    sibling = t + 1 - 2 * (t % 2)
    across = (t + 2) % tp
    diagonal = (sibling + 2) % tp
    other = 1 - r
    rows, own_width = result.shape
    full_width = own_width * tp
    channels = conv_all.shape[2]
    blocks = ug_g.shape[1]
    last = fs - 1
    own_lanes = pl.ds(pl.multiple_of(t * own_width, own_width), own_width)

    sources = (tokens_hbm, outer_hbm, inner_hbm, value_hbm, out_hbm, up_hbm, gate_hbm, down_hbm)
    sources += (mixer_scales_hbm, mixer_taps_hbm, out_scale_hbm, first_gain_hbm.at[:, own_lanes])
    sources += (first_shift_hbm.at[:, own_lanes], up_scales_hbm, ffn_taps_hbm, ffn_shift_hbm, down_scale_hbm)
    sources += (second_gain_hbm.at[:, own_lanes], second_shift_hbm.at[:, own_lanes])
    places = (token_all.at[t], mix_f.at[0], mix_f.at[1], mix_f.at[2], out_f, up_f, gate_f, down_f)
    places += (mixer_scales, mixer_taps, out_scale, first_gain, first_shift, up_scales, ffn_taps, ffn_shift)
    places += (down_scale, second_gain, second_shift)
    loads = [
        pltpu.make_async_copy(source, place, load_sem.at[max(number - 2, min(number, 1))])
        for number, (source, place) in enumerate(zip(sources, places))
    ]
    for load in loads:
        load.start()

    barrier = pltpu.get_barrier_semaphore()
    for peer in (sibling, across, diagonal):
        pl.semaphore_signal(barrier, inc=1, device_id={"tp": peer}, device_id_type=pl.DeviceIdType.MESH)
    pl.semaphore_signal(barrier, inc=1, device_id={"rep": other}, device_id_type=pl.DeviceIdType.MESH)

    @pl.when(z > 0)
    def _():
        pl.semaphore_signal(barrier, inc=1, device_id={"fs": z - 1}, device_id_type=pl.DeviceIdType.MESH)

    @pl.when(z < last)
    def _():
        pl.semaphore_signal(barrier, inc=1, device_id={"fs": z + 1}, device_id_type=pl.DeviceIdType.MESH)

    inside = (z > 0) & (z < last)

    @pl.when(inside)
    def _():
        pl.semaphore_wait(barrier, 6)

    @pl.when(jnp.logical_not(inside))
    def _():
        pl.semaphore_wait(barrier, 5)

    guest_rows = rows // GUEST_PARTS
    return_rows = rows // RETURN_PARTS
    norm_move = 1 + CONV_PARTS
    first_hidden, first_guest = norm_move + 1, norm_move + 1 + blocks * RETURN_PARTS
    conv_rows = rows // CONV_PARTS

    def offset(value, size):
        return value if isinstance(value, int) else pl.multiple_of(value, size)

    def mix_unit(part):
        size = mix_g.shape[1] // (2 * MIX_PARTS)
        return lambda source, half: mix_g.at[source, pl.ds(offset((part * 2 + half) * size, size), size)]

    def out_unit(source, half):
        size = out_g.shape[1] // 2
        return out_g.at[source, pl.ds(offset(half * size, size), size)]

    def ug_unit(block, part):
        size = ug_g.shape[2] // (2 * BLOCK_PARTS[block])
        return lambda source, half: ug_g.at[
            source, block, pl.ds(offset((part * 2 + half) * size, size), size)
        ]

    def down_unit(part):
        size = LANES
        return lambda source, half: down_g.at[source, pl.ds(offset((part * 2 + half) * size, size), size)]

    parts = blocks // 2
    units = [mix_unit(part) for part in range(MIX_PARTS)] + [out_unit]
    out_index, first_down = MIX_PARTS, MIX_PARTS + 1
    units += [down_unit(part) for part in range(parts)]
    first_ug = len(units)
    block_units = []
    for block in range(blocks):
        block_units.append(range(len(units), len(units) + BLOCK_PARTS[block]))
        units += [ug_unit(block, part) for part in range(BLOCK_PARTS[block])]
    count = len(units)

    def program(middle):
        if middle:
            outer, inner, far = (z - 1) * last, last - z, (2 - z) * last
        else:
            near = 1 + z // last
            beyond, far = last - near, last - z
        queues, lowered_blocks = {name: [] for name in LANE_DEPTH}, []
        bases = {}
        for name, depth in LANE_DEPTH.items():
            bases[name] = sum(LANE_DEPTH[other_name] for other_name in bases)

        def send(lane, source, target, recv_sem, device):
            queue, depth = queues[lane], LANE_DEPTH[lane]
            if len(queue) >= depth:
                queue[-depth].wait_send()
            copy = pltpu.make_async_remote_copy(
                src_ref=source,
                dst_ref=target,
                send_sem=send_sem.at[bases[lane] + len(queue) % depth],
                recv_sem=recv_sem,
                device_id=device,
                device_id_type=pl.DeviceIdType.MESH,
            )
            copy.start()
            queue.append(copy)

        def arrived(ref, recv_sem):
            pltpu.make_async_remote_copy(
                src_ref=ref,
                dst_ref=ref,
                send_sem=send_sem.at[0],
                recv_sem=recv_sem,
                device_id={"tp": sibling},
                device_id_type=pl.DeviceIdType.MESH,
            ).wait_recv()

        def moved(number, slot):
            if number == 0:
                return token_all.at[slot]
            if number < norm_move:
                return conv_all.at[slot, pl.ds((number - 1) * conv_rows, conv_rows)]
            if number == norm_move:
                return norm_all.at[slot]
            if number >= first_guest:
                return guest_all.at[slot, pl.ds((number - first_guest) * guest_rows, guest_rows)]
            block, part = (number - first_hidden) // RETURN_PARTS, (number - first_hidden) % RETURN_PARTS
            if middle:
                return hidden_all.at[slot, block]
            return hidden_all.at[slot, block, pl.ds(part * return_rows, return_rows)]

        def exchange_start(number):
            if number == 0:
                loads[0].wait()
            send("x", moved(number, t), moved(number, t), recv_x.at[number, 0], {"tp": across})
            send("d", moved(number, t), moved(number, t), recv_x.at[number, 1], {"tp": sibling})

        def exchange_pass(number):
            arrived(moved(number, across), recv_x.at[number, 0])
            send("d", moved(number, across), moved(number, across), recv_x.at[number, 1], {"tp": sibling})

        def exchange_end(number):
            arrived(moved(number, pl.ds(0, 2)), recv_x.at[number, 1])

        def own(unit):
            ref = units[unit](z, r)
            if middle:
                send("zi", ref, ref, arrive_sem.at[unit, 1], {"fs": inner})
                if unit < first_ug:
                    send("zo", ref, ref, arrive_sem.at[unit, 0], {"fs": outer})
            else:
                send("zi", ref, ref, arrive_sem.at[unit, 0], {"fs": near})

        def own_rest(unit):
            ref = units[unit](z, other)
            send("zi", ref, ref, gather_sem.at[unit], {"fs": near})

        def from_outer(unit):
            ref = units[unit](outer, r)
            arrived(ref, arrive_sem.at[unit, 0])
            send("zi", ref, ref, arrive_sem.at[unit, 2], {"fs": inner})

        def from_inner(unit, source, place):
            ref = units[unit](source, r)
            arrived(ref, arrive_sem.at[unit, place])
            send("y", ref, ref, gather_sem.at[unit], {"rep": other})
            if middle and unit < first_ug:
                send("zo", ref, ref, arrive_sem.at[unit, place], {"fs": outer})

        def need(unit):
            arrived(units[unit](pl.ds(0, 3), 0), gather_sem.at[unit])

        def lower_mix():
            pltpu.make_async_copy(mix_f, mix_f, load_sem.at[1]).wait()
            for part in range(3):
                mix_g[z, :, part * channels : (part + 1) * channels] = mix_f[part].astype(jnp.bfloat16)

        def lower_out():
            loads[4].wait()
            out_g[z] = out_f[...].astype(jnp.bfloat16)

        def lower_down():
            loads[7].wait()
            down_g[z] = down_f[...].astype(jnp.bfloat16)

        def small_loads():
            for load in loads[8:]:
                load.wait()

        def lower_block(block):
            if not lowered_blocks:
                loads[5].wait()
                loads[6].wait()
            lowered_blocks.append(block)
            columns = slice(block * LANES, (block + 1) * LANES)
            ug_g[z, block, :, :LANES] = up_f[:, columns].astype(jnp.bfloat16)
            ug_g[z, block, :, LANES:] = gate_f[:, columns].astype(jnp.bfloat16)

        def sums_start(number, summed):
            lane = lax.broadcasted_iota(jnp.int32, (rows, LANES), 1)
            one = jnp.sum(summed, axis=1, keepdims=True)
            two = jnp.sum(summed * summed, axis=1, keepdims=True)
            stats[number, t] = jnp.transpose(jnp.where(lane == 0, one, two))[:STAT_ROWS]
            ref = stats.at[number, t]
            for lane_name, peer in (("x", across), ("x", diagonal), ("d", sibling)):
                send(lane_name, ref, ref, recv_s.at[number], {"tp": peer})

        def sums_end(number):
            arrived(stats.at[number, pl.ds(0, 3)], recv_s.at[number])
            summed = stats[number, 0]
            for slot in range(1, tp):
                summed = summed + stats[number, slot]
            back = jnp.transpose(jnp.concatenate([summed] * (LANES // STAT_ROWS), axis=0))
            average = back[:, 0:1] / full_width
            return average, back[:, 1:2] / full_width - average * average

        def mixer(part):
            if part == 0:
                for unit in range(MIX_PARTS):
                    need(unit)
                exchange_end(0)
            lines = slice(part * conv_rows, (part + 1) * conv_rows)
            gathered = dot32(token_all[0, lines], mix_g[0])
            for slot in range(1, tp):
                gathered = gathered + dot32(token_all[slot, lines], mix_g[slot])
            scaled = [
                (gathered[:, kind * channels : (kind + 1) * channels] * mixer_scales[kind : kind + 1])
                .astype(jnp.bfloat16)
                .astype(jnp.float32)
                for kind in range(3)
            ]
            mixed = scaled[0] * shifted_mix(
                scaled[1] * scaled[2], mixer_taps[0:1], mixer_taps[1:2], mixer_taps[2:3]
            )
            conv_all[t, lines] = mixed.astype(jnp.bfloat16)
            exchange_start(1 + part)

        def mixer_output():
            need(out_index)
            for part in range(CONV_PARTS):
                exchange_end(1 + part)
            summed = dot32(conv_all[0], out_g[0])
            for slot in range(1, tp):
                summed = summed + dot32(conv_all[slot], out_g[slot])
            summed = summed * out_scale[...] + residual_weight * token_all[t].astype(jnp.float32)
            first_sum[...] = summed
            sums_start(0, summed)

        def first_norm():
            average, spread = sums_end(0)
            norm_all[t] = scaled_norm(
                first_sum[...], average, spread, first_gain[...], first_shift[...]
            ).astype(jnp.bfloat16)

        def guest_send(part):
            lines = pl.ds(part * guest_rows, guest_rows)
            send("zi", norm_all.at[t, lines], guest_all.at[t, lines], recv_g.at[part], {"fs": near})

        def units_of(block, left, lines):
            both = dot32(left(0, lines), ug_g[0, block])
            for slot in range(1, tp):
                both = both + dot32(left(slot, lines), ug_g[slot, block])
            columns = slice(block * LANES, (block + 1) * LANES)
            mixed = []
            for side in range(2):
                mixed.append(
                    shifted_mix(
                        both[:, side * LANES : (side + 1) * LANES] * up_scales[side : side + 1, columns],
                        ffn_taps[0, side : side + 1, columns],
                        ffn_taps[1, side : side + 1, columns],
                        ffn_taps[2, side : side + 1, columns],
                    )
                    + ffn_shift[side : side + 1, columns]
                )
            return (mixed[0] * mixed[1] / (1.0 + jnp.exp(-mixed[1]))).astype(jnp.bfloat16)

        row_cuts = [slice(first, first + ROW_CUT) for first in range(0, rows, ROW_CUT)]

        def store_units(block, left, target):
            for lines in row_cuts:
                target[lines] = units_of(block, lambda slot, lines: left[slot, lines], lines)

        def back_sem(number):
            return arrive_sem.at[first_ug + number // 3, number % 3]

        def need_block(block):
            for unit in block_units[block]:
                need(unit)

        def hidden(block):
            store_units(block, norm_all, hidden_all.at[t, block])
            exchange_start(first_hidden + block * RETURN_PARTS)

        def give_back(block):
            for part in range(RETURN_PARTS):
                lines = pl.ds(part * return_rows, return_rows)
                number = block * RETURN_PARTS + part
                send(
                    "zo", hidden_out.at[block, lines], hidden_all.at[t, block, lines], back_sem(number), {"fs": outer}
                )

        def guest_hidden(block):
            store_units(block, guest_all, hidden_out.at[block])
            give_back(block)

        def both_hidden(block):
            store_units(block, guest_all, hidden_out.at[block])
            store_units(block, norm_all, hidden_all.at[t, block])
            give_back(block)
            exchange_start(first_hidden + block * RETURN_PARTS)

        def guest_start(part):
            lines = pl.ds(part * guest_rows, guest_rows)
            arrived(guest_all.at[t, lines], recv_g.at[part])
            exchange_start(first_guest + part)

        def returned(number):
            arrived(moved(first_hidden + number, t), back_sem(number))
            exchange_start(first_hidden + number)

        def hidden_end(block):
            for part in range(1 if middle else RETURN_PARTS):
                exchange_end(first_hidden + block * RETURN_PARTS + part)

        def down(part):
            need(first_down + part)
            for block in (2 * part, 2 * part + 1):
                hidden_end(block)
            summed = None
            for slot in range(tp):
                left = jnp.concatenate([hidden_all[slot, 2 * part], hidden_all[slot, 2 * part + 1]], axis=1)
                term = dot32(left, down_g[slot, part * 2 * LANES : (part + 1) * 2 * LANES])
                summed = term if summed is None else summed + term
            total[...] = summed if part == 0 else total[...] + summed

        def finish():
            second = total[...] * down_scale[...] + residual_weight * norm_all[t].astype(jnp.float32)
            total[...] = second
            sums_start(1, second)
            average, spread = sums_end(1)
            result[...] = scaled_norm(total[...], average, spread, second_gain[...], second_shift[...]).astype(
                result.dtype
            )
            for name, queue in queues.items():
                for copy in queue[-LANE_DEPTH[name] :]:
                    copy.wait_send()

        if middle:
            lower_mix()
            own(1)
            own(2)
            lower_out()
            exchange_start(0)
            lower_down()
            own(0)
            lower_block(2)
            own(3)
            lower_block(1)
            from_outer(0)
            from_inner(1, inner, 1)
            from_outer(3)
            from_inner(2, inner, 1)
            from_inner(0, inner, 1)
            from_outer(1)
            own(4)
            from_outer(2)
            from_inner(3, far, 2)
            lower_block(4)
            from_outer(4)
            own(9)
            from_inner(1, far, 2)
            from_inner(0, far, 2)
            from_inner(3, inner, 1)
            own(12)
            from_inner(2, far, 2)
            lower_block(3)
            from_inner(4, far, 2)
            small_loads()
            from_inner(4, inner, 1)
            lower_block(0)
            own(5)
            exchange_pass(0)
            from_outer(7)
            from_inner(9, inner, 1)
            mixer(0)
            mixer(1)
            own(6)
            from_outer(9)
            from_inner(12, inner, 1)
            exchange_pass(1)
            own(7)
            exchange_pass(2)
            from_inner(5, inner, 1)
            mixer_output()
            from_inner(7, far, 2)
            from_inner(6, inner, 1)
            from_outer(8)
            first_norm()
            exchange_start(3)
            from_inner(9, far, 2)
            from_outer(5)
            lower_block(5)
            own(8)
            from_outer(10)
            from_inner(7, inner, 1)
            from_inner(8, far, 2)
            from_inner(5, far, 2)
            guest_start(2)
            from_inner(8, inner, 1)
            from_outer(6)
            own(10)
            from_outer(11)
            guest_start(0)
            exchange_pass(3)
            guest_start(1)
            from_inner(10, far, 2)
            from_inner(6, far, 2)
            own(11)
            guest_start(3)
            exchange_pass(16)
            from_inner(10, inner, 1)
            exchange_pass(18)
            exchange_pass(17)
            from_outer(12)
            from_outer(14)
            from_inner(11, far, 2)
            exchange_pass(19)
            from_outer(13)
            exchange_end(3)
            need_block(0)
            from_inner(11, inner, 1)
            exchange_end(18)
            need_block(1)
            exchange_end(16)
            exchange_end(19)
            exchange_end(17)
            guest_hidden(0)
            hidden(1)
            own(14)
            need_block(2)
            from_inner(12, far, 2)
            guest_hidden(1)
            own(13)
            hidden(0)
            from_inner(14, far, 2)
            guest_hidden(2)
            from_inner(13, far, 2)
            need_block(3)
            hidden(2)
            from_inner(14, inner, 1)
            from_inner(13, inner, 1)
            guest_hidden(3)
            need_block(4)
            hidden(4)
            guest_hidden(4)
            exchange_pass(6)
            hidden(3)
            need_block(5)
            exchange_pass(4)
            guest_hidden(5)
            exchange_pass(8)
            hidden(5)
            down(0)
            exchange_pass(10)
            exchange_pass(12)
            exchange_pass(14)
            down(1)
            down(2)
            finish()
        else:
            lower_mix()
            own(0)
            own(3)
            small_loads()
            own(1)
            lower_out()
            lower_down()
            own(2)
            own(4)
            own(7)
            exchange_start(0)
            lower_block(0)
            own_rest(2)
            from_inner(2, near, 0)
            from_inner(0, near, 0)
            lower_block(1)
            from_inner(1, near, 0)
            lower_block(4)
            own_rest(3)
            lower_block(5)
            from_inner(1, beyond, 1)
            own_rest(1)
            own_rest(4)
            own_rest(0)
            from_inner(3, near, 0)
            own(9)
            own(6)
            from_inner(2, beyond, 1)
            own(8)
            from_inner(0, beyond, 1)
            own(12)
            from_inner(3, far, 2)
            from_inner(1, far, 2)
            from_inner(0, far, 2)
            exchange_pass(0)
            from_inner(3, beyond, 1)
            own(5)
            lower_block(3)
            from_inner(2, far, 2)
            from_inner(4, far, 2)
            mixer(0)
            mixer(1)
            lower_block(2)
            own(10)
            from_inner(4, beyond, 1)
            from_inner(4, near, 0)
            exchange_pass(1)
            own(11)
            exchange_pass(2)
            mixer_output()
            first_norm()
            guest_send(2)
            guest_send(0)
            guest_send(1)
            own(14)
            guest_send(3)
            own(13)
            own_rest(8)
            own_rest(9)
            own_rest(10)
            own_rest(11)
            from_inner(5, near, 0)
            from_inner(5, beyond, 1)
            from_inner(7, beyond, 1)
            own_rest(12)
            own_rest(13)
            returned(0)
            from_inner(6, near, 0)
            own_rest(14)
            from_inner(6, beyond, 1)
            own_rest(6)
            returned(1)
            returned(2)
            returned(3)
            returned(4)
            from_inner(7, near, 0)
            returned(5)
            exchange_pass(4)
            from_inner(5, far, 2)
            own_rest(5)
            returned(6)
            own_rest(7)
            from_inner(7, far, 2)
            returned(7)
            exchange_pass(7)
            exchange_pass(5)
            from_inner(6, far, 2)
            returned(8)
            returned(9)
            exchange_pass(6)
            returned(10)
            returned(11)
            exchange_pass(9)
            exchange_pass(14)
            exchange_pass(13)
            exchange_pass(8)
            exchange_pass(11)
            exchange_pass(10)
            exchange_pass(12)
            down(0)
            exchange_pass(15)
            down(1)
            down(2)
            finish()
    @pl.when(inside)
    def _():
        program(True)

    @pl.when(jnp.logical_not(inside))
    def _():
        program(False)


def fused(
    fs,
    tp,
    tokens,
    outer_gate,
    inner_gate,
    mixer_value,
    mixer_scales,
    mixer_taps,
    mixer_out,
    out_scale,
    first_gain,
    first_shift,
    up_proj,
    gate_proj,
    up_scales,
    ffn_taps,
    ffn_shift,
    down_proj,
    down_scale,
    second_gain,
    second_shift,
):
    rows, own_width = tokens.shape
    depth, channels = outer_gate.shape
    hidden = up_proj.shape[1]
    blocks = hidden // LANES
    count = MIX_PARTS + 1 + blocks // 2 + sum(BLOCK_PARTS)
    moves = 2 + CONV_PARTS + blocks * RETURN_PARTS + GUEST_PARTS
    any_space = pl.BlockSpec(memory_space=pl.ANY)
    in_vmem = pl.BlockSpec(memory_space=pltpu.VMEM)

    def row(vector):
        return vector.reshape(1, -1)

    return pl.pallas_call(
        functools.partial(kernel, fs, tp),
        out_shape=jax.ShapeDtypeStruct((rows, own_width), jnp.bfloat16),
        in_specs=[any_space] * 19,
        out_specs=in_vmem,
        scratch_shapes=[
            pltpu.VMEM((3, depth, channels), jnp.float32),
            pltpu.VMEM(mixer_out.shape, jnp.float32),
            pltpu.VMEM(up_proj.shape, jnp.float32),
            pltpu.VMEM(gate_proj.shape, jnp.float32),
            pltpu.VMEM(down_proj.shape, jnp.float32),
            pltpu.VMEM(mixer_scales.shape, jnp.float32),
            pltpu.VMEM(mixer_taps.shape, jnp.float32),
            pltpu.VMEM((1, own_width), jnp.float32),
            pltpu.VMEM((1, own_width), jnp.float32),
            pltpu.VMEM((1, own_width), jnp.float32),
            pltpu.VMEM(up_scales.shape, jnp.float32),
            pltpu.VMEM(ffn_taps.shape, jnp.float32),
            pltpu.VMEM(ffn_shift.shape, jnp.float32),
            pltpu.VMEM((1, own_width), jnp.float32),
            pltpu.VMEM((1, own_width), jnp.float32),
            pltpu.VMEM((1, own_width), jnp.float32),
            pltpu.VMEM((fs, depth, 3 * channels), jnp.bfloat16),
            pltpu.VMEM((fs,) + mixer_out.shape, jnp.bfloat16),
            pltpu.VMEM((fs, blocks, depth, 2 * LANES), jnp.bfloat16),
            pltpu.VMEM((fs,) + down_proj.shape, jnp.bfloat16),
            pltpu.VMEM((tp, rows, own_width), jnp.bfloat16),
            pltpu.VMEM((tp, rows, channels), jnp.bfloat16),
            pltpu.VMEM((tp, rows, own_width), jnp.bfloat16),
            pltpu.VMEM((tp, rows, own_width), jnp.bfloat16),
            pltpu.VMEM((tp, blocks, rows, LANES), jnp.bfloat16),
            pltpu.VMEM((blocks, rows, LANES), jnp.bfloat16),
            pltpu.VMEM((rows, own_width), jnp.float32),
            pltpu.VMEM((rows, own_width), jnp.float32),
            pltpu.VMEM((2, tp, STAT_ROWS, rows), jnp.float32),
            pltpu.SemaphoreType.DMA((17,)),
            pltpu.SemaphoreType.DMA((sum(LANE_DEPTH.values()),)),
            pltpu.SemaphoreType.DMA((count, 3)),
            pltpu.SemaphoreType.DMA((count,)),
            pltpu.SemaphoreType.DMA((moves, 2)),
            pltpu.SemaphoreType.DMA((2,)),
            pltpu.SemaphoreType.DMA((GUEST_PARTS,)),
        ],
        compiler_params=pltpu.CompilerParams(
            collective_id=0, has_side_effects=True, vmem_limit_bytes=60 * 1024 * 1024
        ),
    )(
        tokens,
        outer_gate,
        inner_gate,
        mixer_value,
        mixer_out,
        up_proj,
        gate_proj,
        down_proj,
        mixer_scales,
        mixer_taps,
        row(out_scale),
        row(first_gain),
        row(first_shift),
        up_scales,
        ffn_taps,
        ffn_shift,
        row(down_scale),
        row(second_gain),
        row(second_shift),
    )


def fits(mesh):
    return mesh.shape["rep"] == 2 and mesh.shape["fs"] == 4 and mesh.shape["tp"] == 4


def solution(mesh):
    body = functools.partial(fused, mesh.shape["fs"], mesh.shape["tp"]) if fits(mesh) else local
    return jax.shard_map(
        body,
        mesh=mesh,
        in_specs=(
            P(("rep", "fs"), "tp"),
            P("fs", "tp"),
            P("fs", "tp"),
            P("fs", "tp"),
            P(None, "tp"),
            P(None, "tp"),
            P("fs", "tp"),
            P("tp"),
            P(),
            P(),
            P("fs", "tp"),
            P("fs", "tp"),
            P(None, "tp"),
            P(None, None, "tp"),
            P(None, "tp"),
            P("fs", "tp"),
            P("tp"),
            P(),
            P(),
        ),
        out_specs=P(("rep", "fs"), "tp"),
        check_vma=False,
    )
```
